512 devices in a mesh: sp: 64 (over z, y), tp: 8 (over x, core).
Axes of the slice: x: 4, y: 8, z: 8, core: 2. Of those that a mesh axis runs over, the one named last changes fastest.
Arguments:
- residual: bfloat16 [10240, 2048], P('sp'), may hold values from -6 to 6
- queries: bfloat16 [10240, 8, 128], P('sp', 'tp'), may hold values from -6 to 6
- key_vectors: bfloat16 [10240, 8, 128], P('sp', 'tp'), may hold values from -6 to 6
- value_vecs: bfloat16 [10240, 8, 128], P('sp', 'tp'), may hold values from -6 to 6
- lambda_head: float32 [8], P('tp'), may hold values from 0.3 to 0.8
- head_gain: bfloat16 [128], replicated, may hold values from 0.099609375 to 1.8984375
- w_out: bfloat16 [1024, 2048], P('tp'), may hold values from -0.1875 to 0.1875
- mlp_gain: bfloat16 [2048], replicated, may hold values from 0.099609375 to 1.8984375
- w_gate: bfloat16 [2048, 5632], P('sp', 'tp'), may hold values from -0.125 to 0.125
- w_up: bfloat16 [2048, 5632], P('sp', 'tp'), may hold values from -0.125 to 0.125
- w_down: bfloat16 [5632, 2048], P('tp', 'sp'), may hold values from -0.078125 to 0.078125
Outputs:
- layer_out: bfloat16 [10240, 2048], P(('sp', 'tp'))
The draws below stay inside these ranges and needn't reach their ends.
All inputs are finite; a program needn't handle non-finite values.
Results may differ from the reference program's by a relative error of at most 0.014.
Values may be sent and summed in bfloat16 or wider, within the bound.
A program may use at most 128 MiB of HBM per device.

```python
import math
import jax
import jax.numpy as jnp
from jax import lax

D = 2048
HEADS = 8
QK = 64
HD = 128
FF = 5632
TOKENS = 10240
N_TP = 8


def base_draw(key, salt_value):
    sub_key = jax.random.fold_in(key, salt_value)
    return jnp.clip(1.3 * jax.random.normal(sub_key, (TOKENS, HEADS, 2 * QK), jnp.float32), -6.0, 6.0)


def draw_queries(key, part):
    drawn_vals = base_draw(key, 1)
    return drawn_vals.astype(jnp.bfloat16)


def draw_key_vectors(key, part):
    drawn_vals = base_draw(key, 2)
    return drawn_vals.astype(jnp.bfloat16)


def steps_of(stream_key, extent, cuts, low, largest):
    level = 1.0
    for dim, blocks in cuts:
        draws = jax.random.uniform(jax.random.fold_in(jax.random.fold_in(stream_key, 6), dim), (blocks,), jnp.float32, low / len(cuts), largest / len(cuts))
        level = level * jnp.repeat(jnp.exp(draws), extent[dim] // blocks).reshape((-1,) + (1,) * (len(extent) - 1 - dim))
    return level


def gaussian(stream_key, extent, spread, bound, pieces=(), kind=jnp.bfloat16):
    values = jax.random.normal(stream_key, extent, jnp.float32) * spread
    if len(pieces) > 0:
        values = steps_of(stream_key, extent, pieces, -0.22, 0.18) * values
    return jnp.clip(values, min=-bound, max=bound).astype(kind)


def setup_inputs(seed: int = 0) -> dict:
    splits = jax.random.split(jax.random.key(seed), 12)
    return {
        "residual": gaussian(splits[0], (TOKENS, D), 1.0, 6.0, ((0, 64),)),
        "queries": draw_queries(jax.random.fold_in(splits[11], 71), 0),
        "key_vectors": draw_key_vectors(jax.random.fold_in(splits[11], 71), 0),
        "value_vecs": gaussian(splits[3], (TOKENS, HEADS, HD), 1.0, 6.0, ((0, 64), (1, 8))),
        "lambda_head": jnp.clip(0.3 + 0.5 * jax.random.uniform(splits[4], (HEADS,), jnp.float32) ** steps_of(splits[4], (HEADS,), ((0, 8),), -0.2, 0.2), 0.3, 0.8),
        "head_gain": jnp.clip(1.0 + 0.18 * jax.random.normal(splits[5], (HD,), jnp.float32), 0.099609375, 1.8984375).astype(jnp.bfloat16),
        "w_out": gaussian(splits[6], (HEADS * HD, D), (HEADS * HD) ** -0.5, 0.1875, ((0, 8),)),
        "mlp_gain": jnp.clip(1.0 + 0.18 * jax.random.normal(splits[7], (D,), jnp.float32), 0.099609375, 1.8984375).astype(jnp.bfloat16),
        "w_gate": gaussian(splits[8], (D, FF), D ** -0.5, 0.125, ((0, 64), (1, 8))),
        "w_up": gaussian(splits[9], (D, FF), D ** -0.5, 0.125, ((0, 64), (1, 8))),
        "w_down": gaussian(splits[10], (FF, D), FF ** -0.5, 0.078125, ((0, 8), (1, 64))),
    }


def rms_rows(matrix, gain_vec):
    floats = matrix.astype(jnp.float32)
    scaled = floats * lax.rsqrt(lax.optimization_barrier(jnp.mean(floats * floats, axis=-1, keepdims=True)) + 1e-06)
    return scaled * gain_vec.astype(jnp.float32)

def reference(residual, queries, key_vectors, value_vecs, lambda_head, head_gain, w_out, mlp_gain, w_gate, w_up, w_down):
    row_block = math.gcd(TOKENS, 256)
    score_scale = 1.0 / math.sqrt(QK)
    key_pos = jnp.arange(TOKENS, dtype=jnp.int32)
    key_float = key_vectors.astype(jnp.float32)
    value_float = value_vecs.astype(jnp.float32)

    def attend(block_index):
        begin_row = (block_index * row_block).astype(jnp.int32)
        query_blk = lax.dynamic_slice_in_dim(queries, begin_row, row_block, 0).astype(jnp.float32)
        query_pos = begin_row + jnp.arange(row_block, dtype=jnp.int32)
        causal = key_pos[None, :] <= query_pos[:, None]
        read_out = []
        for member in range(2):
            lower_col = member * QK
            scores = jnp.einsum('qhd,khd->hqk', query_blk[:, :, lower_col:lower_col + QK], key_float[:, :, lower_col:lower_col + QK]) * score_scale
            scores = jnp.where(causal[None], scores, -jnp.inf)
            peak_score = lax.optimization_barrier(jnp.max(scores, axis=-1, keepdims=True))
            weights = jnp.exp(scores - peak_score)
            totals = lax.optimization_barrier(jnp.sum(weights, axis=-1))
            rounded = lax.optimization_barrier(weights.astype(jnp.bfloat16)).astype(jnp.float32)
            acc_sum = jnp.einsum('hqk,khe->hqe', rounded, value_float)
            read_out.append(acc_sum / totals[..., None])
        difference = read_out[0] - lambda_head.astype(jnp.float32)[:, None, None] * read_out[1]
        normed_heads = rms_rows(difference, head_gain)
        return jnp.transpose(normed_heads, (1, 0, 2)).astype(jnp.bfloat16)
    heads_all = lax.map(attend, jnp.arange(TOKENS // row_block, dtype=jnp.int32)).reshape(TOKENS, HEADS * HD)
    group_width = HEADS // N_TP * HD
    projected = jnp.zeros((TOKENS, D), jnp.float32)
    for group in range(N_TP):
        partial_value = jnp.dot(heads_all[:, group * group_width:(group + 1) * group_width], w_out[group * group_width:(group + 1) * group_width], preferred_element_type=jnp.float32)
        projected = projected + partial_value.astype(jnp.bfloat16).astype(jnp.float32)
    middle = (residual.astype(jnp.float32) + projected).astype(jnp.bfloat16)
    normed = rms_rows(middle, mlp_gain).astype(jnp.bfloat16)
    hidden_width = FF // N_TP
    down_sum = jnp.zeros((TOKENS, D), jnp.float32)
    for group in range(N_TP):
        lower_col = group * hidden_width
        gate_act = jnp.dot(normed, w_gate[:, lower_col:lower_col + hidden_width], preferred_element_type=jnp.float32)
        up_act = jnp.dot(normed, w_up[:, lower_col:lower_col + hidden_width], preferred_element_type=jnp.float32)
        hidden = (jax.nn.silu(gate_act) * up_act).astype(jnp.bfloat16)
        partial_value = jnp.dot(hidden, w_down[lower_col:lower_col + hidden_width], preferred_element_type=jnp.float32)
        down_sum = down_sum + partial_value.astype(jnp.bfloat16).astype(jnp.float32)
    return (middle.astype(jnp.float32) + 0.5 * down_sum).astype(jnp.bfloat16)
```

```python
import functools

import jax
import jax.numpy as jnp
from jax import lax
from jax.experimental import pallas as pl
from jax.experimental.pallas import tpu as pltpu
from jax.sharding import PartitionSpec as P

MESH = pl.DeviceIdType.MESH
RING = 8
ROWS = 160
SHARE = 20
WIDTH = 128
MODEL = 2048
GATED = 1408
PACKED = 2176
FAR = -1e30
DIRS = (1, -1)
HALF_STEPS = {1: 4, -1: 3}


def wrap(v):
    return lax.rem(v + 2 * RING, RING)


def nt_dot(a, b, precision=None):
    return lax.dot_general(
        a, b, (((1,), (1,)), ((), ())), preferred_element_type=jnp.float32, precision=precision
    )


def layer(
    lam_ref, resid_hbm, q_ref, k_ref, v_ref, hgain_ref, wo_hbm, mgain_ref, shard_hbm, out_ref,
    weights, wo_all, qg, kg, vext, o_send, o_recv, st_send, st_recv, heads_out, heads_all,
    resid, mid, normed, hidden, piece, own_mid, d_send, d_recv,
    ring1_send, ring1_recv, ring2_send, ring2_recv, q_ss, q_rs, k_ss, k_rs, v_ss, v_rs,
    o_ss, o_rs, st_ss, st_rs, wo_ss, wo_rs, core_ss, core_rs, h_ss, h_rs, d_ss, d_rs, local_sem,
):
    sp = lax.axis_index("sp")
    tp = lax.axis_index("tp")
    z = lax.div(sp, RING)
    y = lax.rem(sp, RING)

    def at_zy(zz, yy):
        return {"sp": zz * RING + yy}

    def remote(src, dst, ss, rs, device):
        return pltpu.make_async_remote_copy(
            src_ref=src, dst_ref=dst, send_sem=ss, recv_sem=rs, device_id=device, device_id_type=MESH
        )

    qg[y] = q_ref[...]
    kg[z] = k_ref[...]
    vext[z, :, 0:WIDTH] = v_ref[...]
    vext[:, :, WIDTH : 2 * WIDTH] = jnp.ones((RING, ROWS, WIDTH), jnp.bfloat16)

    barrier = pltpu.get_barrier_semaphore()
    for j in range(1, RING):
        pl.semaphore_signal(barrier, inc=1, device_id=at_zy(z, wrap(y + j)), device_id_type=MESH)
        pl.semaphore_signal(barrier, inc=1, device_id=at_zy(wrap(z + j), y), device_id_type=MESH)
        pl.semaphore_signal(barrier, inc=1, device_id={"tp": wrap(tp + j)}, device_id_type=MESH)

    local_shard = [
        pltpu.make_async_copy(shard_hbm.at[h], weights.at[z, y, h], local_sem.at[h]) for h in range(2)
    ]
    local_resid = pltpu.make_async_copy(resid_hbm, resid, local_sem.at[2])
    local_wo = pltpu.make_async_copy(wo_hbm, wo_all.at[tp], local_sem.at[3])
    for c in local_shard + [local_resid, local_wo]:
        c.start()
    pl.semaphore_wait(barrier, 3 * (RING - 1))

    def q_copy(j, src_slot):
        return remote(q_ref, qg.at[src_slot], q_ss.at[j], q_rs.at[j], at_zy(z, wrap(y + j + 1)))

    def k_copy(j, src_slot):
        return remote(k_ref, kg.at[src_slot], k_ss.at[j], k_rs.at[j], at_zy(wrap(z + j + 1), y))

    def v_copy(j, src_slot):
        return remote(
            v_ref, vext.at[src_slot, :, pl.ds(0, WIDTH)], v_ss.at[j], v_rs.at[j], at_zy(wrap(z + j + 1), y)
        )

    for j in (0, 6, 1, 5, 2, 4, 3):
        k_copy(j, z).start()
        v_copy(j, z).start()
        q_copy(j, y).start()

    def ring1(h, d, k, arriving=False):
        back = k if arriving else k - 1
        if h == 0:
            slot = weights.at[z, wrap(y - d * back), 0]
            device = at_zy(z, wrap(y + d))
        else:
            slot = weights.at[wrap(z - d * back), y, 1]
            device = at_zy(wrap(z + d), y)
        index = (h * 2 + (d < 0)) * 4 + k - 1
        src = shard_hbm.at[h] if (k == 1 and not arriving) else slot
        return remote(src, slot, ring1_send.at[index], ring1_recv.at[index], device)

    def ring2_steps(d, sub):
        return HALF_STEPS[d] if sub == 0 else HALF_STEPS[-d]

    def ring2(h, d, sub, k, arriving=False):
        back = k if arriving else k - 1
        if h == 0:
            slot = weights.at[wrap(z - d * back), pl.ds(4 * sub, 4), 0]
            device = at_zy(wrap(z + d), y)
        else:
            slot = weights.at[pl.ds(4 * sub, 4), wrap(y - d * back), 1]
            device = at_zy(z, wrap(y + d))
        index = ((h * 2 + (d < 0)) * 2 + sub) * 4 + k - 1
        return remote(slot, slot, ring2_send.at[index], ring2_recv.at[index], device)

    def wo_copy(j, slot):
        return remote(wo_hbm, wo_all.at[slot], wo_ss.at[j], wo_rs.at[j], {"tp": wrap(tp + 2 * (j + 1))})

    partner = tp + 1 - 2 * lax.rem(tp, 2)

    def core_copy(j, slot):
        return remote(wo_all.at[slot], wo_all.at[slot], core_ss.at[j], core_rs.at[j], {"tp": partner})

    for h in range(2):
        for d in DIRS:
            ring1(h, d, 1).start()
    for j in (0, 2, 1):
        wo_copy(j, tp).start()

    for k in range(1, 5):
        for d in DIRS:
            for h in range(2):
                if k <= HALF_STEPS[d]:
                    ring1(h, d, k, True).wait_recv()
                    if k < HALF_STEPS[d]:
                        ring1(h, d, k + 1).start()
    for c in local_shard:
        c.wait()

    for sub in range(2):
        for h in range(2):
            for d in DIRS:
                ring2(h, d, sub, 1).start()

    def ring2_forward(sub, k):
        for h in range(2):
            for d in DIRS:
                if k <= ring2_steps(d, sub):
                    ring2(h, d, sub, k, True).wait_recv()
                    if k < ring2_steps(d, sub):
                        ring2(h, d, sub, k + 1).start()

    for j in range(7):
        q_copy(j, wrap(y - j - 1)).wait_recv()
        k_copy(j, wrap(z - j - 1)).wait_recv()
        v_copy(j, wrap(z - j - 1)).wait_recv()

    lane = lax.broadcasted_iota(jnp.int32, (ROWS, WIDTH), 1)
    key_lane = lax.broadcasted_iota(jnp.int32, (1, RING * ROWS), 1)
    key_pos = key_lane + y * ROWS
    for j in range(1, RING):
        key_pos = key_pos + jnp.where(key_lane >= j * ROWS, (RING - 1) * ROWS, 0)
    row_iota = lax.broadcasted_iota(jnp.int32, (ROWS, 1), 0)
    pick = (
        lax.broadcasted_iota(jnp.int32, (8, WIDTH), 1) == 64 * lax.broadcasted_iota(jnp.int32, (8, WIDTH), 0)
    ).astype(jnp.float32)
    spread = (
        lax.div(lax.broadcasted_iota(jnp.int32, (8, 2 * WIDTH), 1), WIDTH)
        == lax.broadcasted_iota(jnp.int32, (8, 2 * WIDTH), 0)
    ).astype(jnp.float32)

    def o_copy(i, src_slot):
        return remote(o_send.at[i], o_recv.at[src_slot], o_ss.at[i], o_rs.at[i], at_zy(z, wrap(y + i + 1)))

    def st_copy(i, src_slot):
        return remote(st_send.at[i], st_recv.at[src_slot], st_ss.at[i], st_rs.at[i], at_zy(z, wrap(y + i + 1)))

    def attend(i, own):
        yq = y if own else wrap(y + i + 1)
        q = qg[yq] * jnp.bfloat16(0.125)
        q_pos = z * (RING * ROWS) + yq * ROWS + row_iota
        seen = key_pos <= q_pos
        keys = kg[...].reshape(RING * ROWS, WIDTH)
        vals = vext[...].reshape(RING * ROWS, 2 * WIDTH)
        logs = []
        for m in range(2):
            half = (lane < 64) if m == 0 else (lane >= 64)
            qm = jnp.where(half, q.astype(jnp.float32), 0.0).astype(jnp.bfloat16)
            s = jnp.where(seen, nt_dot(qm, keys), FAR)
            top = jnp.max(s, axis=1, keepdims=True)
            p = jnp.exp(s - top).astype(jnp.bfloat16)
            both = jnp.dot(p, vals, preferred_element_type=jnp.float32)
            total = both[:, WIDTH:]
            reading = (both[:, :WIDTH] / total).astype(jnp.bfloat16)
            if own:
                o_recv[y, m] = reading
            else:
                o_send[i, m] = reading
            logs.append(top + jnp.log(total))
        stats = nt_dot(pick, jnp.where(lane < 64, logs[0], logs[1]), lax.Precision.HIGHEST)
        if own:
            st_recv[y] = stats
        else:
            st_send[i] = stats
            o_copy(i, y).start()
            st_copy(i, y).start()

    def attend_step(i, carry):
        attend(i, False)
        return carry

    lax.fori_loop(0, 4, attend_step, 0)
    ring2_forward(0, 1)
    lax.fori_loop(4, 7, attend_step, 0)
    attend(7, True)
    ring2_forward(1, 1)

    local_wo.wait()
    for j in range(3):
        wo_copy(j, wrap(tp - 2 * (j + 1))).wait_recv()
    for j in range(4):
        core_copy(j, wrap(tp + 2 * j)).start()

    for i in range(7):
        o_copy(i, wrap(y - i - 1)).wait_recv()
        st_copy(i, wrap(y - i - 1)).wait_recv()

    stat = [lax.dot_general(st_recv[p], spread, (((0,), (0,)), ((), ())), preferred_element_type=jnp.float32,
                            precision=lax.Precision.HIGHEST) for p in range(RING)]
    readings = []
    for m in range(2):
        ls = [s[:, m * WIDTH : (m + 1) * WIDTH] for s in stat]
        top = functools.reduce(jnp.maximum, ls)
        share = [jnp.exp(l - top) for l in ls]
        total = functools.reduce(jnp.add, share)
        acc = functools.reduce(jnp.add, [share[p] * o_recv[p, m].astype(jnp.float32) for p in range(RING)])
        readings.append(acc / total)
    diff = readings[0] - lam_ref[0] * readings[1]
    scale = lax.rsqrt(jnp.mean(diff * diff, axis=1, keepdims=True) + 1e-06)
    heads = (diff * scale * hgain_ref[...].astype(jnp.float32)).astype(jnp.bfloat16)
    heads_out[...] = heads

    def h_copy(j, slot):
        lanes = pl.ds(pl.multiple_of(slot * WIDTH, WIDTH), WIDTH)
        return remote(heads_out, heads_all.at[:, lanes], h_ss.at[j], h_rs.at[j], {"tp": wrap(tp + j + 1)})

    for j in range(7):
        h_copy(j, tp).start()
    heads_all[:, pl.ds(pl.multiple_of(tp * WIDTH, WIDTH), WIDTH)] = heads
    ring2_forward(0, 2)
    local_resid.wait()
    for j in range(4):
        core_copy(j, wrap(partner + 2 * j)).wait_recv()
    for j in range(7):
        h_copy(j, wrap(tp - j - 1)).wait_recv()

    def project(c, squares):
        lanes = pl.ds(pl.multiple_of(c * 256, 256), 256)
        w = wo_all[:, :, lanes].reshape(RING * WIDTH, 256)
        part = jnp.dot(heads_all[...], w, preferred_element_type=jnp.float32)
        m = (resid[:, lanes].astype(jnp.float32) + part).astype(jnp.bfloat16).astype(jnp.float32)
        mid[:, lanes] = m
        return squares + m[:, :WIDTH] * m[:, :WIDTH] + m[:, WIDTH:] * m[:, WIDTH:]

    squares = lax.fori_loop(0, 8, project, jnp.zeros((ROWS, WIDTH), jnp.float32))
    scale = lax.rsqrt(jnp.sum(squares, axis=1, keepdims=True) * (1.0 / MODEL) + 1e-06)

    def norm(c, carry):
        lanes = pl.ds(pl.multiple_of(c * 256, 256), 256)
        normed[:, lanes] = (mid[:, lanes] * scale * mgain_ref[:, lanes].astype(jnp.float32)).astype(jnp.bfloat16)
        return carry

    lax.fori_loop(0, 8, norm, 0)
    for t in range(RING):
        @pl.when(tp == t)
        def _():
            own_mid[...] = mid[t * SHARE : (t + 1) * SHARE, :]

    ring2_forward(1, 2)
    ring2_forward(0, 3)
    ring2_forward(1, 3)
    ring2_forward(0, 4)
    ring2_forward(1, 4)

    def silu_times(g, u):
        return (g / (1.0 + jnp.exp(-g)) * u).astype(jnp.bfloat16)

    def gate_up(c, carry):
        lanes = pl.ds(pl.multiple_of(c * 256, 256), 256)
        w = weights[:, :, :, :, lanes].reshape(MODEL, 256)
        r = jnp.dot(normed[...], w, preferred_element_type=jnp.float32)
        hidden[:, pl.ds(pl.multiple_of(c * WIDTH, WIDTH), WIDTH)] = silu_times(r[:, :WIDTH], r[:, WIDTH:])
        return carry

    lax.fori_loop(0, 5, gate_up, 0)
    w = weights[:, :, :, :, GATED - WIDTH : GATED].reshape(MODEL, WIDTH)
    r = jnp.dot(normed[...], w, preferred_element_type=jnp.float32)
    r = jnp.where(lane < 64, silu_times(r, pltpu.roll(r, 64, 1)).astype(jnp.float32), 0.0)
    hidden[:, 5 * WIDTH :] = r.astype(jnp.bfloat16)

    def d_copy(j, part, dst_slot, device):
        lanes = pl.ds(part * (MODEL // 2), MODEL // 2)
        peer = wrap(tp + j + 1)
        index = part * 7 + j
        return remote(d_send.at[peer, :, lanes], d_recv.at[dst_slot, :, lanes], d_ss.at[index], d_rs.at[index],
                      {"tp": peer})

    def down(c, carry):
        w = weights[c, :, :, :, GATED:PACKED].reshape(256, PACKED - GATED)
        lanes = pl.ds(pl.multiple_of(c * 256, 256), 256)
        piece[...] = nt_dot(hidden[...], w)
        for t in range(RING):
            d_send[t, :, lanes] = piece[t * SHARE : (t + 1) * SHARE, :].astype(jnp.bfloat16)
        return carry

    for part in range(2):
        lax.fori_loop(4 * part, 4 * part + 4, down, 0)
        for j in range(7):
            d_copy(j, part, tp, None).start()

    d_recv[tp] = d_send[tp]
    for part in range(2):
        for j in range(7):
            d_copy(j, part, wrap(tp - j - 1), None).wait_recv()
    total = functools.reduce(jnp.add, [d_recv[t].astype(jnp.float32) for t in range(RING)])
    out_ref[...] = (own_mid[...] + 0.5 * total).astype(jnp.bfloat16)

    for j in range(7):
        q_copy(j, y).wait_send()
        k_copy(j, z).wait_send()
        v_copy(j, z).wait_send()
        o_copy(j, y).wait_send()
        st_copy(j, y).wait_send()
        h_copy(j, tp).wait_send()
        for part in range(2):
            d_copy(j, part, tp, None).wait_send()
    for j in range(3):
        wo_copy(j, tp).wait_send()
    for j in range(4):
        core_copy(j, wrap(tp + 2 * j)).wait_send()
    for h in range(2):
        for d in DIRS:
            for k in range(1, HALF_STEPS[d] + 1):
                ring1(h, d, k).wait_send()
            for sub in range(2):
                for k in range(1, ring2_steps(d, sub) + 1):
                    ring2(h, d, sub, k).wait_send()


def local(residual, queries, key_vectors, value_vecs, lambda_head, head_gain, w_out, mlp_gain, w_gate, w_up, w_down):
    depth = w_gate.shape[0]
    main = jnp.stack(
        [w_gate[:, :640].reshape(depth, 5, WIDTH), w_up[:, :640].reshape(depth, 5, WIDTH)], axis=2
    ).reshape(depth, 1280)
    packed = jnp.concatenate(
        [main, w_gate[:, 640:], w_up[:, 640:], w_down.T, jnp.zeros((depth, 64), jnp.bfloat16)], axis=1
    ).reshape(2, depth // 2, PACKED)
    vmem = pl.BlockSpec(memory_space=pltpu.VMEM)
    hbm = pl.BlockSpec(memory_space=pl.ANY)
    dma = pltpu.SemaphoreType.DMA
    bf, f32 = jnp.bfloat16, jnp.float32
    return pl.pallas_call(
        layer,
        out_shape=jax.ShapeDtypeStruct((SHARE, MODEL), bf),
        in_specs=[pl.BlockSpec(memory_space=pltpu.SMEM), hbm, vmem, vmem, vmem, vmem, hbm, vmem, hbm],
        out_specs=vmem,
        scratch_shapes=[
            pltpu.VMEM((RING, RING, 2, 16, PACKED), bf),
            pltpu.VMEM((RING, WIDTH, MODEL), bf),
            pltpu.VMEM((RING, ROWS, WIDTH), bf),
            pltpu.VMEM((RING, ROWS, WIDTH), bf),
            pltpu.VMEM((RING, ROWS, 2 * WIDTH), bf),
            pltpu.VMEM((RING - 1, 2, ROWS, WIDTH), bf),
            pltpu.VMEM((RING, 2, ROWS, WIDTH), bf),
            pltpu.VMEM((RING - 1, 8, ROWS), f32),
            pltpu.VMEM((RING, 8, ROWS), f32),
            pltpu.VMEM((ROWS, WIDTH), bf),
            pltpu.VMEM((ROWS, RING * WIDTH), bf),
            pltpu.VMEM((ROWS, MODEL), bf),
            pltpu.VMEM((ROWS, MODEL), f32),
            pltpu.VMEM((ROWS, MODEL), bf),
            pltpu.VMEM((ROWS, PACKED - GATED), bf),
            pltpu.VMEM((ROWS, 256), f32),
            pltpu.VMEM((SHARE, MODEL), f32),
            pltpu.VMEM((RING, SHARE, MODEL), bf),
            pltpu.VMEM((RING, SHARE, MODEL), bf),
            dma((16,)), dma((16,)), dma((32,)), dma((32,)),
            dma((7,)), dma((7,)), dma((7,)), dma((7,)), dma((7,)), dma((7,)),
            dma((7,)), dma((7,)), dma((7,)), dma((7,)),
            dma((3,)), dma((3,)), dma((4,)), dma((4,)), dma((7,)), dma((7,)), dma((14,)), dma((14,)), dma((4,)),
        ],
        compiler_params=pltpu.CompilerParams(
            collective_id=0, has_side_effects=True, vmem_limit_bytes=56 * 1024 * 1024
        ),
    )(
        lambda_head, residual, queries.reshape(ROWS, WIDTH), key_vectors.reshape(ROWS, WIDTH),
        value_vecs.reshape(ROWS, WIDTH), head_gain.reshape(1, WIDTH), w_out, mlp_gain.reshape(1, MODEL), packed,
    )


def solution(mesh):
    in_specs = (
        P("sp", None), P("sp", "tp", None), P("sp", "tp", None), P("sp", "tp", None), P("tp"), P(),
        P("tp", None), P(), P("sp", "tp"), P("sp", "tp"), P("tp", "sp"),
    )
    return jax.shard_map(
        local, mesh=mesh, in_specs=in_specs, out_specs=P(("sp", "tp"), None), check_vma=False
    )
```

```python
import functools

import jax
import jax.numpy as jnp
from jax import lax
from jax.experimental import pallas as pl
from jax.experimental.pallas import tpu as pltpu
from jax.sharding import PartitionSpec as P

MESH = pl.DeviceIdType.MESH
RING = 8
ROWS = 160
SHARE = 20
WIDTH = 128
MODEL = 2048
MAIN = 1280
REST = 896
OFFSETS = (0, 1, -1, 2, -2, 3, -3, 4)
FAR = -1e30
DIRS = (1, -1)
HALF_STEPS = {1: 4, -1: 3}


def hops(offset, d):
    return 4 if (d > 0) == (offset % 2 == 0) else 3


def onward(event):
    kind, d, k = event[0], event[-2], event[-1]
    if kind == "q" or kind == "kv":
        return [(kind, d, k + 1)] if k < HALF_STEPS[d] else []
    if kind == "r1":
        h = event[1]
        more = [("r1", h, d, k + 1)] if k < HALF_STEPS[d] else []
        return more + [("r2", h, d * k, e, 1) for e in DIRS]
    if kind == "r2":
        h, offset = event[1], event[2]
        return [("r2", h, offset, d, k + 1)] if k < hops(offset, d) else []
    return []


def plan():
    rate, latency = 46600.0, 1.9
    sizes = {"q": ROWS * WIDTH * 2, "kv": ROWS * WIDTH * 4}
    wide = (32 * MAIN * 2, 32 * REST * 2)
    free, arrivals, actions = {}, {}, []
    now = 0.0

    def send(event):
        kind, d = event[0], event[-2]
        if kind in sizes:
            size, axis = sizes[kind], kind == "kv"
        else:
            size, axis = wide[event[1]], (event[1] == 1) == (kind == "r1")
        done = max(free.get((axis, d), 0.0), now) + size / rate
        free[(axis, d)] = done
        arrivals[event] = done + latency

    for event in first_sends():
        send(event)
    ready = {"attend": None, "merge": None, "project": None}
    attended, read_at = 0, None
    while arrivals or ready["project"] != "done":
        if ready["attend"] is None and not any(e[0] in sizes for e in arrivals):
            ready["attend"] = now
        block = None
        if ready["attend"] is not None and attended < SEGMENTS:
            block = ("attend", attended, now, 2.5)
        elif attended == SEGMENTS and ready["merge"] != "done":
            block = ("merge", 0, read_at, 2.2)
        elif ready["merge"] == "done" and ready["project"] != "done":
            block = ("project", 0, read_at, 2.7)
        event = min(arrivals, key=lambda e: arrivals[e]) if arrivals else None
        if event is not None and (block is None or arrivals[event] <= max(now, block[2])):
            now = max(now, arrivals.pop(event))
            actions.append(event)
            for more in onward(event):
                send(more)
            continue
        now = max(now, block[2]) + block[3]
        actions.append(block[:2])
        if block[0] == "attend":
            for d in DIRS:
                free[(False, d)] = max(free.get((False, d), 0.0), now) + 8 * ROWS * WIDTH * 4 / rate / SEGMENTS
            attended += 1
            read_at = max(free[(False, d)] for d in DIRS) + 3.0
        else:
            ready[block[0]] = "done"
            read_at = now + 6.0
    return actions, now


def first_sends():
    first = [("kv", d, 1) for d in DIRS] + [("q", d, 1) for d in DIRS]
    first += [("r1", h, d, 1) for h in (1, 0) for d in DIRS]
    return first + [("r2", h, 0, d, 1) for h in (0, 1) for d in DIRS]


SEGMENTS = 4


def wrap(v):
    return lax.rem(v + 2 * RING, RING)


def nt_dot(a, b, precision=None):
    return lax.dot_general(
        a, b, (((1,), (1,)), ((), ())), preferred_element_type=jnp.float32, precision=precision
    )


def layer(
    lam_ref, resid_hbm, q_ref, k_ref, v_ref, hgain_ref, wo_hbm, mgain_ref, gate_ref, up_ref, down_ref, out_ref,
    wa, wb, wo_all, qg, kvg, vext, o_part, o_recv, st_part, st_recv, heads_out, heads_all,
    resid, mid, normed, hidden, piece, own_mid, d_send, d_recv,
    r1_ss, r1_rs, r2_ss, r2_rs, q_ss, q_rs, kv_ss, kv_rs,
    o_ss, o_rs, st_ss, st_rs, wo_ss, wo_rs, core_ss, core_rs, h_ss, h_rs, d_ss, d_rs, local_sem,
):
    sp = lax.axis_index("sp")
    tp = lax.axis_index("tp")
    z = lax.div(sp, RING)
    y = lax.rem(sp, RING)

    def at_zy(zz, yy):
        return {"sp": zz * RING + yy}

    def remote(src, dst, ss, rs, device):
        return pltpu.make_async_remote_copy(
            src_ref=src, dst_ref=dst, send_sem=ss, recv_sem=rs, device_id=device, device_id_type=MESH
        )

    barrier = pltpu.get_barrier_semaphore()
    for d in DIRS:
        pl.semaphore_signal(barrier, inc=1, device_id=at_zy(wrap(z + d), y), device_id_type=MESH)
    for j in range(1, RING):
        pl.semaphore_signal(barrier, inc=1, device_id=at_zy(z, wrap(y + j)), device_id_type=MESH)
        pl.semaphore_signal(barrier, inc=1, device_id={"tp": wrap(tp + j)}, device_id_type=MESH)

    local_resid = pltpu.make_async_copy(resid_hbm, resid, local_sem.at[0])
    local_wo = pltpu.make_async_copy(wo_hbm, wo_all.at[tp], local_sem.at[1])
    local_resid.start()
    local_wo.start()
    qg[y] = q_ref[...]
    kvg[z, 0] = k_ref[...]
    kvg[z, 1] = v_ref[...]
    for c in range(5):
        wa[z, y, :, 256 * c : 256 * c + WIDTH] = gate_ref[:, WIDTH * c : WIDTH * (c + 1)]
        wa[z, y, :, 256 * c + WIDTH : 256 * (c + 1)] = up_ref[:, WIDTH * c : WIDTH * (c + 1)]
    wb[z, y, :, 0:WIDTH] = jnp.concatenate([gate_ref[:, 640:], up_ref[:, 640:]], axis=1)
    wb[z, y, :, WIDTH : 6 * WIDTH] = down_ref[:, :640]
    wb[z, y, :, 6 * WIDTH :] = jnp.concatenate([down_ref[:, 640:], jnp.zeros((32, 64), jnp.bfloat16)], axis=1)
    pl.semaphore_wait(barrier, 2 + 2 * (RING - 1))

    def copy_of(event, arriving=False):
        kind, d, k = event[0], event[-2], event[-1]
        back = k if arriving else k - 1
        if kind == "q":
            slot = qg.at[wrap(y - d * back)]
            index = (d < 0) * 4 + k - 1
            return remote(slot, slot, q_ss.at[index], q_rs.at[index], at_zy(z, wrap(y + d)))
        if kind == "kv":
            slot = kvg.at[wrap(z - d * back)]
            index = (d < 0) * 4 + k - 1
            return remote(slot, slot, kv_ss.at[index], kv_rs.at[index], at_zy(wrap(z + d), y))
        h = event[1]
        buffer = wb if h else wa
        if kind == "r1":
            dz, dy = (d, 0) if h else (0, d)
            slot = buffer.at[wrap(z - dz * back), wrap(y - dy * back)]
            index = (h * 2 + (d < 0)) * 4 + k - 1
            return remote(slot, slot, r1_ss.at[index], r1_rs.at[index], at_zy(wrap(z + dz), wrap(y + dy)))
        offset = event[2]
        if h:
            slot = buffer.at[wrap(z - offset), wrap(y - d * back)]
            device = at_zy(z, wrap(y + d))
        else:
            slot = buffer.at[wrap(z - d * back), wrap(y - offset)]
            device = at_zy(wrap(z + d), y)
        index = ((h * 2 + (d < 0)) * RING + OFFSETS.index(offset)) * 4 + k - 1
        return remote(slot, slot, r2_ss.at[index], r2_rs.at[index], device)

    started = []

    def start(event):
        started.append(event)
        copy_of(event).start()

    for event in first_sends():
        start(event)

    def wo_copy(j, slot):
        return remote(wo_hbm, wo_all.at[slot], wo_ss.at[j], wo_rs.at[j], {"tp": wrap(tp + 2 * (j + 1))})

    partner = tp + 1 - 2 * lax.rem(tp, 2)

    def core_copy(j, slot):
        return remote(wo_all.at[slot], wo_all.at[slot], core_ss.at[j], core_rs.at[j], {"tp": partner})

    for j in (0, 2, 1):
        wo_copy(j, tp).start()
    vext[:, WIDTH:] = jnp.ones((RING * ROWS, WIDTH), jnp.bfloat16)

    lane = lax.broadcasted_iota(jnp.int32, (ROWS, WIDTH), 1)
    key_lane = lax.broadcasted_iota(jnp.int32, (1, RING * ROWS), 1)
    key_pos = key_lane + y * ROWS
    for j in range(1, RING):
        key_pos = key_pos + jnp.where(key_lane >= j * ROWS, (RING - 1) * ROWS, 0)
    row_iota = lax.broadcasted_iota(jnp.int32, (ROWS, 1), 0)
    pick = (
        lax.broadcasted_iota(jnp.int32, (8, WIDTH), 1) == 64 * lax.broadcasted_iota(jnp.int32, (8, WIDTH), 0)
    ).astype(jnp.float32)
    spread = (
        lax.div(lax.broadcasted_iota(jnp.int32, (8, 2 * WIDTH), 1), WIDTH)
        == lax.broadcasted_iota(jnp.int32, (8, 2 * WIDTH), 0)
    ).astype(jnp.float32)

    def far(i):
        return 4 + (i // 2 if i % 2 == 0 else -(i + 1) // 2) if isinstance(i, int) else 4 + jnp.where(
            lax.rem(i, 2) == 0, lax.div(i, 2), -lax.div(i + 1, 2))

    def o_copies(i):
        device = at_zy(z, wrap(y + far(i)))
        return (
            remote(o_part.at[i], o_recv.at[i], o_ss.at[i], o_rs.at[i], device),
            remote(st_part.at[i], st_recv.at[i], st_ss.at[i], st_rs.at[i], device),
        )

    def attend(i, carry):
        yq = wrap(y + far(i))
        q = qg[yq] * jnp.bfloat16(0.125)
        q_pos = z * (RING * ROWS) + yq * ROWS + row_iota
        seen = key_pos <= q_pos
        keys = kvg[:, 0].reshape(RING * ROWS, WIDTH)
        logs = []
        for m in range(2):
            half = (lane < 64) if m == 0 else (lane >= 64)
            qm = jnp.where(half, q.astype(jnp.float32), 0.0).astype(jnp.bfloat16)
            s = jnp.where(seen, nt_dot(qm, keys), FAR)
            top = jnp.max(s, axis=1, keepdims=True)
            p = jnp.exp(s - top).astype(jnp.bfloat16)
            both = jnp.dot(p, vext[...], preferred_element_type=jnp.float32)
            total = both[:, WIDTH:]
            o_part[i, m] = (both[:, :WIDTH] / total).astype(jnp.bfloat16)
            logs.append(top + jnp.log(total))
        st_part[i] = nt_dot(pick, jnp.where(lane < 64, logs[0], logs[1]), lax.Precision.HIGHEST)

        @pl.when(i < RING - 1)
        def _():
            for c in o_copies(i):
                c.start()

        return carry

    def attend_segment(n):
        if n == 0:
            vext[:, :WIDTH] = kvg[:, 1].reshape(RING * ROWS, WIDTH)
        per = RING // SEGMENTS
        lax.fori_loop(n * per, (n + 1) * per, attend, 0)
        if n == SEGMENTS - 1:
            local_wo.wait()
            for j in range(3):
                wo_copy(j, wrap(tp - 2 * (j + 1))).wait_recv()
            for j in range(4):
                core_copy(j, wrap(tp + 2 * j)).start()

    def h_copy(j, slot):
        lanes = pl.ds(pl.multiple_of(slot * WIDTH, WIDTH), WIDTH)
        return remote(heads_out, heads_all.at[:, lanes], h_ss.at[j], h_rs.at[j], {"tp": wrap(tp + j + 1)})

    def merge_heads():
        for i in range(RING - 1):
            for c in o_copies(i):
                c.wait_recv()
        parts = [o_recv.at[i] for i in range(RING - 1)] + [o_part.at[RING - 1]]
        stats = [st_recv[i] for i in range(RING - 1)] + [st_part[RING - 1]]
        stat = [lax.dot_general(st, spread, (((0,), (0,)), ((), ())), preferred_element_type=jnp.float32,
                                precision=lax.Precision.HIGHEST) for st in stats]
        readings = []
        for m in range(2):
            ls = [st[:, m * WIDTH : (m + 1) * WIDTH] for st in stat]
            top = functools.reduce(jnp.maximum, ls)
            share = [jnp.exp(l - top) for l in ls]
            total = functools.reduce(jnp.add, share)
            acc = functools.reduce(jnp.add, [w * o[m].astype(jnp.float32) for w, o in zip(share, parts)])
            readings.append(acc / total)
        diff = readings[0] - lam_ref[0] * readings[1]
        scale = lax.rsqrt(jnp.mean(diff * diff, axis=1, keepdims=True) + 1e-06)
        heads = (diff * scale * hgain_ref[...].astype(jnp.float32)).astype(jnp.bfloat16)
        heads_out[...] = heads
        for j in (2, 3, 4, 1, 5, 0, 6):
            h_copy(j, tp).start()
        heads_all[:, pl.ds(pl.multiple_of(tp * WIDTH, WIDTH), WIDTH)] = heads
        local_resid.wait()

    def project_rows():
        for j in range(4):
            core_copy(j, wrap(partner + 2 * j)).wait_recv()
        for j in range(7):
            h_copy(j, wrap(tp - j - 1)).wait_recv()

        def project(c, squares):
            lanes = pl.ds(pl.multiple_of(c * 256, 256), 256)
            w = wo_all[:, :, lanes].reshape(RING * WIDTH, 256)
            part = jnp.dot(heads_all[...], w, preferred_element_type=jnp.float32)
            m = (resid[:, lanes].astype(jnp.float32) + part).astype(jnp.bfloat16).astype(jnp.float32)
            mid[:, lanes] = m
            return squares + m[:, :WIDTH] * m[:, :WIDTH] + m[:, WIDTH:] * m[:, WIDTH:]

        squares = lax.fori_loop(0, 8, project, jnp.zeros((ROWS, WIDTH), jnp.float32))
        scale = lax.rsqrt(jnp.sum(squares, axis=1, keepdims=True) * (1.0 / MODEL) + 1e-06)

        def norm(c, carry):
            lanes = pl.ds(pl.multiple_of(c * 256, 256), 256)
            normed[:, lanes] = (mid[:, lanes] * scale * mgain_ref[:, lanes].astype(jnp.float32)).astype(jnp.bfloat16)
            return carry

        lax.fori_loop(0, 8, norm, 0)
        for t in range(RING):
            @pl.when(tp == t)
            def _():
                own_mid[...] = mid[t * SHARE : (t + 1) * SHARE, :]

    for action in plan()[0]:
        if action[0] == "attend":
            attend_segment(action[1])
        elif action[0] == "merge":
            merge_heads()
        elif action[0] == "project":
            project_rows()
        else:
            copy_of(action, True).wait_recv()
            for event in onward(action):
                start(event)

    def silu_times(g, u):
        return (g / (1.0 + jnp.exp(-g)) * u).astype(jnp.bfloat16)

    def gate_up(c, carry):
        w = wa[:, :, :, pl.ds(pl.multiple_of(c * 256, 256), 256)].reshape(MODEL, 256)
        r = jnp.dot(normed[...], w, preferred_element_type=jnp.float32)
        hidden[:, pl.ds(pl.multiple_of(c * WIDTH, WIDTH), WIDTH)] = silu_times(r[:, :WIDTH], r[:, WIDTH:])
        return carry

    lax.fori_loop(0, 5, gate_up, 0)
    r = jnp.dot(normed[...], wb[:, :, :, 0:WIDTH].reshape(MODEL, WIDTH), preferred_element_type=jnp.float32)
    r = jnp.where(lane < 64, silu_times(r, pltpu.roll(r, 64, 1)).astype(jnp.float32), 0.0)
    hidden[:, 5 * WIDTH :] = r.astype(jnp.bfloat16)

    def d_copy(j, part, dst_slot):
        lanes = pl.ds(part * (MODEL // 2), MODEL // 2)
        peer = wrap(tp + j + 1)
        index = part * 7 + j
        return remote(d_send.at[peer, :, lanes], d_recv.at[dst_slot, :, lanes], d_ss.at[index], d_rs.at[index],
                      {"tp": peer})

    def down(c, carry):
        w = wb[c, :, :, WIDTH:].reshape(256, REST - WIDTH)
        lanes = pl.ds(pl.multiple_of(c * 256, 256), 256)
        piece[...] = nt_dot(hidden[...], w)
        for t in range(RING):
            d_send[t, :, lanes] = piece[t * SHARE : (t + 1) * SHARE, :].astype(jnp.bfloat16)
        return carry

    for part in range(2):
        lax.fori_loop(4 * part, 4 * part + 4, down, 0)
        for j in (2, 3, 4, 1, 5, 0, 6):
            d_copy(j, part, tp).start()

    d_recv[tp] = d_send[tp]
    for part in range(2):
        for j in range(7):
            d_copy(j, part, wrap(tp - j - 1)).wait_recv()
    total = functools.reduce(jnp.add, [d_recv[t].astype(jnp.float32) for t in range(RING)])
    out_ref[...] = (own_mid[...] + 0.5 * total).astype(jnp.bfloat16)

    for event in started:
        copy_of(event).wait_send()
    for j in range(7):
        for c in o_copies(j):
            c.wait_send()
        h_copy(j, tp).wait_send()
        for part in range(2):
            d_copy(j, part, tp).wait_send()
    for j in range(3):
        wo_copy(j, tp).wait_send()
    for j in range(4):
        core_copy(j, wrap(tp + 2 * j)).wait_send()


def local(residual, queries, key_vectors, value_vecs, lambda_head, head_gain, w_out, mlp_gain, w_gate, w_up, w_down):
    vmem = pl.BlockSpec(memory_space=pltpu.VMEM)
    hbm = pl.BlockSpec(memory_space=pl.ANY)
    dma = pltpu.SemaphoreType.DMA
    bf, f32 = jnp.bfloat16, jnp.float32
    return pl.pallas_call(
        layer,
        out_shape=jax.ShapeDtypeStruct((SHARE, MODEL), bf),
        in_specs=[pl.BlockSpec(memory_space=pltpu.SMEM), hbm, vmem, vmem, vmem, vmem, hbm, vmem, vmem, vmem, vmem],
        out_specs=vmem,
        scratch_shapes=[
            pltpu.VMEM((RING, RING, 32, MAIN), bf),
            pltpu.VMEM((RING, RING, 32, REST), bf),
            pltpu.VMEM((RING, WIDTH, MODEL), bf),
            pltpu.VMEM((RING, ROWS, WIDTH), bf),
            pltpu.VMEM((RING, 2, ROWS, WIDTH), bf),
            pltpu.VMEM((RING * ROWS, 2 * WIDTH), bf),
            pltpu.VMEM((RING, 2, ROWS, WIDTH), bf),
            pltpu.VMEM((RING - 1, 2, ROWS, WIDTH), bf),
            pltpu.VMEM((RING, 8, ROWS), f32),
            pltpu.VMEM((RING - 1, 8, ROWS), f32),
            pltpu.VMEM((ROWS, WIDTH), bf),
            pltpu.VMEM((ROWS, RING * WIDTH), bf),
            pltpu.VMEM((ROWS, MODEL), bf),
            pltpu.VMEM((ROWS, MODEL), f32),
            pltpu.VMEM((ROWS, MODEL), bf),
            pltpu.VMEM((ROWS, REST - WIDTH), bf),
            pltpu.VMEM((ROWS, 256), f32),
            pltpu.VMEM((SHARE, MODEL), f32),
            pltpu.VMEM((RING, SHARE, MODEL), bf),
            pltpu.VMEM((RING, SHARE, MODEL), bf),
            dma((16,)), dma((16,)), dma((128,)), dma((128,)), dma((8,)), dma((8,)), dma((8,)), dma((8,)),
            dma((7,)), dma((7,)), dma((7,)), dma((7,)),
            dma((3,)), dma((3,)), dma((4,)), dma((4,)), dma((7,)), dma((7,)), dma((14,)), dma((14,)), dma((2,)),
        ],
        compiler_params=pltpu.CompilerParams(
            collective_id=0, has_side_effects=True, vmem_limit_bytes=56 * 1024 * 1024
        ),
    )(
        lambda_head, residual, queries.reshape(ROWS, WIDTH), key_vectors.reshape(ROWS, WIDTH),
        value_vecs.reshape(ROWS, WIDTH), head_gain.reshape(1, WIDTH), w_out, mlp_gain.reshape(1, MODEL),
        w_gate, w_up, w_down.T,
    )


def solution(mesh):
    in_specs = (
        P("sp", None), P("sp", "tp", None), P("sp", "tp", None), P("sp", "tp", None), P("tp"), P(),
        P("tp", None), P(), P("sp", "tp"), P("sp", "tp"), P("tp", "sp"),
    )
    return jax.shard_map(
        local, mesh=mesh, in_specs=in_specs, out_specs=P(("sp", "tp"), None), check_vma=False
    )
```

```python
import functools

import jax
import jax.numpy as jnp
from jax import lax
from jax.experimental import pallas as pl
from jax.experimental.pallas import tpu as pltpu
from jax.sharding import PartitionSpec as P

MESH = pl.DeviceIdType.MESH
RING = 8
ROWS = 160
SHARE = 20
WIDTH = 128
MODEL = 2048
FAR = -1e30
DIRS = (1, -1)
STEPS = {1: 4, -1: 3}
SPREAD = {1: 3, -1: 4}
OFFSETS = (0, 1, -1, 2, -2, 3, -3, -4)
SEGMENTS = 8
LIMIT = 3.25
PIECES = ((0, 768), (1, 640), (0, 512), (1, 256))


def hops(offset, d):
    return 4 if (d > 0) == (offset % 2 == 0) else 3


def onward(event):
    kind, d, k = event[0], event[-2], event[-1]
    if kind in ("q", "kv"):
        return [(kind, d, k + 1)] if k < STEPS[d] else []
    if kind == "r1":
        more = [("r1", event[1], d, k + 1)] if k < SPREAD[d] else []
        return more + [("r2", event[1], d * k, e, 1) for e in DIRS]
    return [event[:-1] + (k + 1,)] if k < hops(event[2], d) else []


def over_z(event):
    if event[0] in ("q", "kv"):
        return event[0] == "kv"
    return (PIECES[event[1]][0] == 1) == (event[0] == "r1")


def column_of(event):
    if event[0] not in ("r1", "r2") or event[1] < 2:
        return None
    travel = event[-2] * event[-1]
    along_z = travel if over_z(event) else (event[2] if event[0] == "r2" else 0)
    return along_z % RING


def plan(limit):
    rate, latency = 46600.0, 1.9
    free, arrivals, actions, held = {}, {}, [], []
    now = 0.0
    missing = {r: (14 if r == 0 else 16) for r in range(RING)}
    gated = 2 * (RING * RING - 1)

    def rank(event):
        return 0 if event[0] in ("q", "kv") else 1 + 2 * (event[1] // 2) + (event[0] == "r2")

    def size(event):
        if event[0] in ("q", "kv"):
            return ROWS * WIDTH * (2 if event[0] == "q" else 4)
        return 64 * PIECES[event[1]][1]

    def release():
        for event in sorted(held, key=rank):
            link = (over_z(event), event[-2])
            if rank(event) == 0 or free.get(link, 0.0) - now <= limit:
                held.remove(event)
                free[link] = max(free.get(link, 0.0), now) + size(event) / rate
                arrivals[event] = free[link] + latency
                actions.append(("start", event))

    for d in DIRS:
        held += [("kv", d, 1), ("q", d, 1)]
    for p in range(4):
        held += [("r1", p, d, 1) for d in DIRS] + [("r2", p, 0, d, 1) for d in DIRS]
    release()
    attended, stage, at = 0, "attend", None
    rows = []
    while arrivals or held or stage != "end":
        if stage == "attend" and at is None and not any(e[0] in ("q", "kv") for e in list(arrivals) + held):
            at = now
        ready = None
        if stage == "gate_up":
            ready = now if gated == 0 else None
        elif stage == "down":
            ready = now if any(missing[r] == 0 and r not in rows for r in range(RING)) else None
        elif stage != "end":
            ready = at
        event = min(arrivals, key=lambda e: arrivals[e]) if arrivals else None
        if event is not None and (ready is None or arrivals[event] <= max(now, ready)):
            now = max(now, arrivals.pop(event))
            actions.append(("wait", event))
            held += onward(event)
            if column_of(event) is not None:
                missing[column_of(event)] -= 1
            elif event[0] in ("r1", "r2"):
                gated -= 1
        elif ready is None:
            now += 0.3
        else:
            now = max(now, ready)
            if stage == "attend":
                now += 1.3
                actions.append(("attend", attended))
                attended += 1
                for d in DIRS:
                    link = (False, d)
                    free[link] = max(free.get(link, 0.0), now) + ROWS * WIDTH * 4 * RING / SEGMENTS / rate
                if attended == SEGMENTS:
                    stage, at = "merge", max(free[(False, d)] for d in DIRS) + 3.0
            elif stage == "merge":
                now += 2.0
                actions.append(("merge", 0))
                stage, at = "project", now + 5.0
            elif stage == "project":
                now += 2.6
                actions.append(("project", 0))
                stage = "gate_up"
            elif stage == "gate_up":
                now += 2.3
                actions.append(("gate_up", 0))
                stage = "down"
            else:
                row = [r for r in range(RING) if missing[r] == 0 and r not in rows][0]
                now += 0.4
                actions.append(("down", row))
                rows.append(row)
                if len(rows) == RING:
                    stage = "end"
        release()
    return actions, now


def wrap(v):
    return lax.rem(v + 2 * RING, RING)


def nt_dot(a, b, precision=None):
    return lax.dot_general(
        a, b, (((1,), (1,)), ((), ())), preferred_element_type=jnp.float32, precision=precision
    )


def layer(
    lam_ref, resid_hbm, q_ref, k_ref, v_ref, hgain_ref, wo_hbm, mgain_ref, gate_ref, up_ref, down_ref, out_ref,
    w0, w1, w2, w3, wo_all, qg, kvg, vext, o_part, o_recv, st_part, st_recv, heads_out, heads_all,
    resid, mid, normed, hidden, piece, own_mid, d_send, d_recv,
    r1_ss, r1_rs, r2_ss, r2_rs, q_ss, q_rs, kv_ss, kv_rs,
    o_ss, o_rs, st_ss, st_rs, wo_ss, wo_rs, core_ss, core_rs, h_ss, h_rs, d_ss, d_rs, local_sem,
):
    sp = lax.axis_index("sp")
    tp = lax.axis_index("tp")
    z = lax.div(sp, RING)
    y = lax.rem(sp, RING)

    def at_zy(zz, yy):
        return {"sp": zz * RING + yy}

    def remote(src, dst, ss, rs, device):
        return pltpu.make_async_remote_copy(
            src_ref=src, dst_ref=dst, send_sem=ss, recv_sem=rs, device_id=device, device_id_type=MESH
        )

    barrier = pltpu.get_barrier_semaphore()
    for d in DIRS:
        pl.semaphore_signal(barrier, inc=1, device_id=at_zy(wrap(z + d), y), device_id_type=MESH)
    for j in range(1, RING):
        pl.semaphore_signal(barrier, inc=1, device_id=at_zy(z, wrap(y + j)), device_id_type=MESH)
        pl.semaphore_signal(barrier, inc=1, device_id={"tp": wrap(tp + j)}, device_id_type=MESH)

    local_resid = pltpu.make_async_copy(resid_hbm, resid, local_sem.at[0])
    local_wo = pltpu.make_async_copy(wo_hbm, wo_all.at[tp], local_sem.at[1])
    local_resid.start()
    local_wo.start()
    qg[y] = q_ref[...]
    kvg[z, 0] = k_ref[...]
    kvg[z, 1] = v_ref[...]
    for c in range(5):
        pair = w0.at[z, y, :, pl.ds(256 * c, 256)] if c < 3 else w1.at[z, y, :, pl.ds(256 * (c - 3), 256)]
        pair[:, 0:WIDTH] = gate_ref[:, WIDTH * c : WIDTH * (c + 1)]
        pair[:, WIDTH:] = up_ref[:, WIDTH * c : WIDTH * (c + 1)]
    w1[z, y, :, 512:] = jnp.concatenate([gate_ref[:, 640:], up_ref[:, 640:]], axis=1)
    w2[z, y] = down_ref[:, :512]
    w3[z, y, :, :WIDTH] = down_ref[:, 512:640]
    w3[z, y, :, WIDTH:] = jnp.concatenate([down_ref[:, 640:], jnp.zeros((32, 64), jnp.bfloat16)], axis=1)
    pl.semaphore_wait(barrier, 2 + 2 * (RING - 1))

    def copy_of(event, arriving=False):
        kind, d, k = event[0], event[-2], event[-1]
        back = k if arriving else k - 1
        if kind == "q":
            slot = qg.at[wrap(y - d * back)]
            index = (d < 0) * 4 + k - 1
            return remote(slot, slot, q_ss.at[index], q_rs.at[index], at_zy(z, wrap(y + d)))
        if kind == "kv":
            slot = kvg.at[wrap(z - d * back)]
            index = (d < 0) * 4 + k - 1
            return remote(slot, slot, kv_ss.at[index], kv_rs.at[index], at_zy(wrap(z + d), y))
        p = event[1]
        buffer = (w0, w1, w2, w3)[p]
        first_z = PIECES[p][0]
        if kind == "r1":
            dz, dy = (d, 0) if first_z else (0, d)
            slot = buffer.at[wrap(z - dz * back), wrap(y - dy * back)]
            index = (p * 2 + (d < 0)) * 4 + k - 1
            return remote(slot, slot, r1_ss.at[index], r1_rs.at[index], at_zy(wrap(z + dz), wrap(y + dy)))
        offset = event[2]
        if first_z:
            slot = buffer.at[wrap(z - offset), wrap(y - d * back)]
            device = at_zy(z, wrap(y + d))
        else:
            slot = buffer.at[wrap(z - d * back), wrap(y - offset)]
            device = at_zy(wrap(z + d), y)
        index = ((p * 2 + (d < 0)) * RING + OFFSETS.index(offset)) * 4 + k - 1
        return remote(slot, slot, r2_ss.at[index], r2_rs.at[index], device)

    started = []

    def start(event):
        started.append(event)
        copy_of(event).start()

    def wo_copy(j, slot):
        return remote(wo_hbm, wo_all.at[slot], wo_ss.at[j], wo_rs.at[j], {"tp": wrap(tp + 2 * (j + 1))})

    partner = tp + 1 - 2 * lax.rem(tp, 2)

    def core_copy(j, slot):
        return remote(wo_all.at[slot], wo_all.at[slot], core_ss.at[j], core_rs.at[j], {"tp": partner})

    for j in (0, 2, 1):
        wo_copy(j, tp).start()
    vext[:, WIDTH:] = jnp.ones((RING * ROWS, WIDTH), jnp.bfloat16)

    lane = lax.broadcasted_iota(jnp.int32, (ROWS, WIDTH), 1)
    key_lane = lax.broadcasted_iota(jnp.int32, (1, RING * ROWS), 1)
    key_pos = key_lane + y * ROWS
    for j in range(1, RING):
        key_pos = key_pos + jnp.where(key_lane >= j * ROWS, (RING - 1) * ROWS, 0)
    row_iota = lax.broadcasted_iota(jnp.int32, (ROWS, 1), 0)
    pick = (
        lax.broadcasted_iota(jnp.int32, (8, WIDTH), 1) == 64 * lax.broadcasted_iota(jnp.int32, (8, WIDTH), 0)
    ).astype(jnp.float32)
    spread = (
        lax.div(lax.broadcasted_iota(jnp.int32, (8, 2 * WIDTH), 1), WIDTH)
        == lax.broadcasted_iota(jnp.int32, (8, 2 * WIDTH), 0)
    ).astype(jnp.float32)

    def far(i):
        return 4 + (i // 2 if i % 2 == 0 else -(i + 1) // 2) if isinstance(i, int) else 4 + jnp.where(
            lax.rem(i, 2) == 0, lax.div(i, 2), -lax.div(i + 1, 2))

    def o_copies(i):
        device = at_zy(z, wrap(y + far(i)))
        return (
            remote(o_part.at[i], o_recv.at[i], o_ss.at[i], o_rs.at[i], device),
            remote(st_part.at[i], st_recv.at[i], st_ss.at[i], st_rs.at[i], device),
        )

    def attend(i, carry):
        yq = wrap(y + far(i))
        q = qg[yq] * jnp.bfloat16(0.125)
        q_pos = z * (RING * ROWS) + yq * ROWS + row_iota
        seen = key_pos <= q_pos
        keys = kvg[:, 0].reshape(RING * ROWS, WIDTH)
        logs = []
        for m in range(2):
            half = (lane < 64) if m == 0 else (lane >= 64)
            qm = jnp.where(half, q.astype(jnp.float32), 0.0).astype(jnp.bfloat16)
            s = jnp.where(seen, nt_dot(qm, keys), FAR)
            top = jnp.max(s, axis=1, keepdims=True)
            p = jnp.exp(s - top).astype(jnp.bfloat16)
            both = jnp.dot(p, vext[...], preferred_element_type=jnp.float32)
            total = both[:, WIDTH:]
            o_part[i, m] = (both[:, :WIDTH] / total).astype(jnp.bfloat16)
            logs.append(top + jnp.log(total))
        st_part[i] = nt_dot(pick, jnp.where(lane < 64, logs[0], logs[1]), lax.Precision.HIGHEST)

        @pl.when(i < RING - 1)
        def _():
            for c in o_copies(i):
                c.start()

        return carry

    def attend_segment(n):
        if n == 0:
            vext[:, :WIDTH] = kvg[:, 1].reshape(RING * ROWS, WIDTH)
        per = RING // SEGMENTS
        lax.fori_loop(n * per, (n + 1) * per, attend, 0)
        if n == SEGMENTS - 1:
            local_wo.wait()
            for j in range(3):
                wo_copy(j, wrap(tp - 2 * (j + 1))).wait_recv()
            for j in range(4):
                core_copy(j, wrap(tp + 2 * j)).start()

    def h_copy(j, slot):
        lanes = pl.ds(pl.multiple_of(slot * WIDTH, WIDTH), WIDTH)
        return remote(heads_out, heads_all.at[:, lanes], h_ss.at[j], h_rs.at[j], {"tp": wrap(tp + j + 1)})

    def merge_heads():
        for i in range(RING - 1):
            for c in o_copies(i):
                c.wait_recv()
        parts = [o_recv.at[i] for i in range(RING - 1)] + [o_part.at[RING - 1]]
        stats = [st_recv[i] for i in range(RING - 1)] + [st_part[RING - 1]]
        stat = [lax.dot_general(st, spread, (((0,), (0,)), ((), ())), preferred_element_type=jnp.float32,
                                precision=lax.Precision.HIGHEST) for st in stats]
        readings = []
        for m in range(2):
            ls = [st[:, m * WIDTH : (m + 1) * WIDTH] for st in stat]
            top = functools.reduce(jnp.maximum, ls)
            share = [jnp.exp(l - top) for l in ls]
            total = functools.reduce(jnp.add, share)
            acc = functools.reduce(jnp.add, [w * o[m].astype(jnp.float32) for w, o in zip(share, parts)])
            readings.append(acc / total)
        diff = readings[0] - lam_ref[0] * readings[1]
        scale = lax.rsqrt(jnp.mean(diff * diff, axis=1, keepdims=True) + 1e-06)
        heads = (diff * scale * hgain_ref[...].astype(jnp.float32)).astype(jnp.bfloat16)
        heads_out[...] = heads
        for j in (2, 3, 4, 1, 5, 0, 6):
            h_copy(j, tp).start()
        heads_all[:, pl.ds(pl.multiple_of(tp * WIDTH, WIDTH), WIDTH)] = heads
        local_resid.wait()

    def project_rows():
        for j in range(4):
            core_copy(j, wrap(partner + 2 * j)).wait_recv()
        for j in range(7):
            h_copy(j, wrap(tp - j - 1)).wait_recv()

        def project(c, squares):
            lanes = pl.ds(pl.multiple_of(c * 256, 256), 256)
            w = wo_all[:, :, lanes].reshape(RING * WIDTH, 256)
            part = jnp.dot(heads_all[...], w, preferred_element_type=jnp.float32)
            m = (resid[:, lanes].astype(jnp.float32) + part).astype(jnp.bfloat16).astype(jnp.float32)
            mid[:, lanes] = m
            return squares + m[:, :WIDTH] * m[:, :WIDTH] + m[:, WIDTH:] * m[:, WIDTH:]

        squares = lax.fori_loop(0, 8, project, jnp.zeros((ROWS, WIDTH), jnp.float32))
        scale = lax.rsqrt(jnp.sum(squares, axis=1, keepdims=True) * (1.0 / MODEL) + 1e-06)

        def norm(c, carry):
            lanes = pl.ds(pl.multiple_of(c * 256, 256), 256)
            normed[:, lanes] = (mid[:, lanes] * scale * mgain_ref[:, lanes].astype(jnp.float32)).astype(jnp.bfloat16)
            return carry

        lax.fori_loop(0, 8, norm, 0)
        for t in range(RING):
            @pl.when(tp == t)
            def _():
                own_mid[...] = mid[t * SHARE : (t + 1) * SHARE, :]

    def silu_times(g, u):
        return (g / (1.0 + jnp.exp(-g)) * u).astype(jnp.bfloat16)

    def gated_rows():
        for buffer, first, pairs in ((w0, 0, 3), (w1, 3, 2)):
            def gate_up(c, carry):
                w = buffer[:, :, :, pl.ds(pl.multiple_of(c * 256, 256), 256)].reshape(MODEL, 256)
                r = jnp.dot(normed[...], w, preferred_element_type=jnp.float32)
                lanes = pl.ds(pl.multiple_of((c + first) * WIDTH, WIDTH), WIDTH)
                hidden[:, lanes] = silu_times(r[:, :WIDTH], r[:, WIDTH:])
                return carry

            lax.fori_loop(0, pairs, gate_up, 0)
        r = jnp.dot(normed[...], w1[:, :, :, 512:].reshape(MODEL, WIDTH), preferred_element_type=jnp.float32)
        r = jnp.where(lane < 64, silu_times(r, pltpu.roll(r, 64, 1)).astype(jnp.float32), 0.0)
        hidden[:, 5 * WIDTH :] = r.astype(jnp.bfloat16)

    def d_copy(j, turn, row):
        lanes = pl.ds(pl.multiple_of(wrap(z - row) * 256, 256), 256)
        peer = wrap(tp + j + 1)
        index = turn * 7 + j
        return remote(d_send.at[peer, :, lanes], d_recv.at[j, :, lanes], d_ss.at[index], d_rs.at[index], {"tp": peer})

    def down_row(turn, row):
        slot = wrap(z - row)
        lanes = pl.ds(pl.multiple_of(slot * 256, 256), 256)
        piece[...] = nt_dot(hidden[:, 0:512], w2[slot].reshape(256, 512)) + nt_dot(
            hidden[:, 512:], w3[slot].reshape(256, 256)
        )
        for t in range(RING):
            d_send[t, :, lanes] = piece[t * SHARE : (t + 1) * SHARE, :].astype(jnp.bfloat16)
        for j in (2, 3, 4, 1, 5, 0, 6):
            d_copy(j, turn, row).start()

    turns = []
    for kind, what in plan(LIMIT)[0]:
        if kind == "attend":
            attend_segment(what)
        elif kind == "merge":
            merge_heads()
        elif kind == "project":
            project_rows()
        elif kind == "gate_up":
            gated_rows()
        elif kind == "down":
            down_row(len(turns), what)
            turns.append(what)
        elif kind == "wait":
            copy_of(what, True).wait_recv()
        else:
            start(what)

    for turn, row in enumerate(turns):
        for j in range(7):
            d_copy(j, turn, row).wait_recv()
    total = functools.reduce(jnp.add, [d_recv[j].astype(jnp.float32) for j in range(RING - 1)])
    total = total + d_send[tp].astype(jnp.float32)
    out_ref[...] = (own_mid[...] + 0.5 * total).astype(jnp.bfloat16)

    for event in started:
        copy_of(event).wait_send()
    for j in range(7):
        for c in o_copies(j):
            c.wait_send()
        h_copy(j, tp).wait_send()
        for turn, row in enumerate(turns):
            d_copy(j, turn, row).wait_send()
    for j in range(3):
        wo_copy(j, tp).wait_send()
    for j in range(4):
        core_copy(j, wrap(tp + 2 * j)).wait_send()


def local(residual, queries, key_vectors, value_vecs, lambda_head, head_gain, w_out, mlp_gain, w_gate, w_up, w_down):
    vmem = pl.BlockSpec(memory_space=pltpu.VMEM)
    hbm = pl.BlockSpec(memory_space=pl.ANY)
    dma = pltpu.SemaphoreType.DMA
    bf, f32 = jnp.bfloat16, jnp.float32
    return pl.pallas_call(
        layer,
        out_shape=jax.ShapeDtypeStruct((SHARE, MODEL), bf),
        in_specs=[pl.BlockSpec(memory_space=pltpu.SMEM), hbm, vmem, vmem, vmem, vmem, hbm, vmem, vmem, vmem, vmem],
        out_specs=vmem,
        scratch_shapes=[
            *[pltpu.VMEM((RING, RING, 32, lanes), bf) for _, lanes in PIECES],
            pltpu.VMEM((RING, WIDTH, MODEL), bf),
            pltpu.VMEM((RING, ROWS, WIDTH), bf),
            pltpu.VMEM((RING, 2, ROWS, WIDTH), bf),
            pltpu.VMEM((RING * ROWS, 2 * WIDTH), bf),
            pltpu.VMEM((RING, 2, ROWS, WIDTH), bf),
            pltpu.VMEM((RING - 1, 2, ROWS, WIDTH), bf),
            pltpu.VMEM((RING, 8, ROWS), f32),
            pltpu.VMEM((RING - 1, 8, ROWS), f32),
            pltpu.VMEM((ROWS, WIDTH), bf),
            pltpu.VMEM((ROWS, RING * WIDTH), bf),
            pltpu.VMEM((ROWS, MODEL), bf),
            pltpu.VMEM((ROWS, MODEL), f32),
            pltpu.VMEM((ROWS, MODEL), bf),
            pltpu.VMEM((ROWS, 6 * WIDTH), bf),
            pltpu.VMEM((ROWS, 256), f32),
            pltpu.VMEM((SHARE, MODEL), f32),
            pltpu.VMEM((RING, SHARE, MODEL), bf),
            pltpu.VMEM((RING - 1, SHARE, MODEL), bf),
            dma((32,)), dma((32,)), dma((256,)), dma((256,)), dma((8,)), dma((8,)), dma((8,)), dma((8,)),
            dma((7,)), dma((7,)), dma((7,)), dma((7,)),
            dma((3,)), dma((3,)), dma((4,)), dma((4,)), dma((7,)), dma((7,)), dma((56,)), dma((56,)), dma((2,)),
        ],
        compiler_params=pltpu.CompilerParams(
            collective_id=0, has_side_effects=True, vmem_limit_bytes=56 * 1024 * 1024
        ),
    )(
        lambda_head, residual, queries.reshape(ROWS, WIDTH), key_vectors.reshape(ROWS, WIDTH),
        value_vecs.reshape(ROWS, WIDTH), head_gain.reshape(1, WIDTH), w_out, mlp_gain.reshape(1, MODEL),
        w_gate, w_up, w_down.T,
    )


def solution(mesh):
    in_specs = (
        P("sp", None), P("sp", "tp", None), P("sp", "tp", None), P("sp", "tp", None), P("tp"), P(),
        P("tp", None), P(), P("sp", "tp"), P("sp", "tp"), P("tp", "sp"),
    )
    return jax.shard_map(
        local, mesh=mesh, in_specs=in_specs, out_specs=P(("sp", "tp"), None), check_vma=False
    )
```

```python
import functools
import itertools

import jax
import jax.numpy as jnp
from jax import lax
from jax.experimental import pallas as pl
from jax.experimental.pallas import tpu as pltpu
from jax.sharding import PartitionSpec as P

MESH = pl.DeviceIdType.MESH
RING = 8
ROWS = 160
SHARE = 20
WIDTH = 128
MODEL = 2048
FAR = -1e30
DIRS = (1, -1)
STEPS = {1: 4, -1: 3}
SPREAD = {1: 3, -1: 4}
OFFSETS = (0, 1, -1, 2, -2, 3, -3, -4)
TURNS = ((1, 1), (-1, 1), (1, 2), (-1, 2), (1, 3), (-1, 3), (1, 4), (0, 0))
LIMITS = (1.8, 1.8, 2.5, 2.0)
PAIRS, DOWN = 3, 3
PIECES = ((0, 256 * PAIRS), (1, 1408 - 256 * PAIRS), (0, 128 * DOWN), (1, 768 - 128 * DOWN))


def hops(offset, d):
    return 4 if (d > 0) == (offset % 2 == 0) else 3


def onward(event):
    kind, d, k = event[0], event[-2], event[-1]
    if kind == "o":
        return []
    if kind in ("q", "kv"):
        return [(kind, d, k + 1)] if k < STEPS[d] else []
    if kind == "r1":
        more = [("r1", event[1], d, k + 1)] if k < SPREAD[d] else []
        return more + [("r2", event[1], d * k, e, 1) for e in DIRS]
    return [event[:-1] + (k + 1,)] if k < hops(event[2], d) else []


def last_gate(event):
    return event[0] == "r2" and event[1] < 2 and event[-1] == hops(event[2], event[3])


def own_flags():
    events = [("r1", p, d, k) for p in range(4) for d in DIRS for k in range(1, SPREAD[d] + 1)]
    events += [
        ("r2", p, o, d, k) for p in range(4) for o in OFFSETS for d in DIRS for k in range(1, hops(o, d) + 1)
    ]
    return {e: i for i, e in enumerate(e for e in events if not last_gate(e))}


def over_z(event):
    if event[0] in ("q", "kv", "o"):
        return event[0] == "kv"
    return (PIECES[event[1]][0] == 1) == (event[0] == "r1")


def column_of(event):
    if event[0] not in ("r1", "r2") or event[1] < 2:
        return None
    travel = event[-2] * event[-1]
    along_z = travel if over_z(event) else (event[2] if event[0] == "r2" else 0)
    return along_z % RING


def plan(limits):
    rate, latency = 46600.0, 2.2
    free, arrivals, actions, held = {}, {}, [], []
    now = 0.0
    missing = {r: (14 if r == 0 else 16) for r in range(RING)}
    gated = 2 * (RING * RING - 1)

    def rank(event):
        return 0 if event[0] in ("q", "kv", "o") else 1 + 2 * (event[1] // 2) + (event[0] == "r2")

    def size(event):
        if event[0] in ("q", "kv", "o"):
            return ROWS * WIDTH * (2 if event[0] == "q" else 4)
        return 64 * PIECES[event[1]][1]

    def release():
        for event in sorted(held, key=rank):
            link = (over_z(event), event[-2])
            if stage == "attend" and at is not None and not link[0]:
                calm = limits[1]
            else:
                calm = limits[3] if rank(event) > 2 else limits[0] if at is None else limits[2]
            if rank(event) == 0 or free.get(link, 0.0) - now <= calm:
                held.remove(event)
                free[link] = max(free.get(link, 0.0), now) + size(event) / rate
                arrivals[event] = free[link] + latency
                actions.append(("start", event))

    for d in DIRS:
        held += [("kv", d, 1), ("q", d, 1)]
    for p in range(4):
        held += [("r1", p, d, 1) for d in DIRS] + [("r2", p, 0, d, 1) for d in DIRS]
    attended, passed, stage, at, sent = 0, 0, "attend", None, 0.0
    release()
    came, rows = set(), []
    while arrivals or held or stage != "end":
        if at is None and not any(e[0] in ("q", "kv") for e in list(arrivals) + held):
            at = now
        block = None
        if stage == "attend" and at is not None:
            d, k = TURNS[passed]
            needed = {("o", 1, 4), ("o", -1, 3)} if d == 0 else {("o", d, k - 1)} if k > 1 else set()
            if passed < attended and needed <= came:
                block = ("merge", 0, 1.2) if d == 0 else ("pass", passed, 0.4)
            elif attended < len(TURNS):
                block = ("attend", attended, 1.3)
        elif stage == "project":
            block = ("project", 0, 2.6)
        elif stage == "gate_up" and gated == 0:
            block = ("gate_up", 0, 2.3)
        elif stage == "down":
            done = [r for r in range(RING) if missing[r] == 0 and r not in rows]
            if len(done) > 1:
                block = ("down", (done[0], done[1]), 0.8)
        ready = None if block is None else max(now, at) if stage == "project" else now
        event = min(arrivals, key=lambda e: arrivals[e]) if arrivals else None
        if event is not None and (block is None or arrivals[event] <= ready):
            now = max(now, arrivals.pop(event))
            actions.append(("wait", event))
            came.add(event)
            held += onward(event)
            if column_of(event) is not None:
                missing[column_of(event)] -= 1
            elif event[0] in ("r1", "r2"):
                gated -= 1
        elif block is None:
            now += 0.3
        else:
            now = ready + block[2]
            actions.append(block[:2])
            if block[0] == "attend":
                attended += 1
            elif block[0] == "pass":
                held.append(("o",) + TURNS[passed])
                passed += 1
            elif block[0] == "merge":
                stage, at = "project", now + 5.0
            elif block[0] == "project":
                stage = "gate_up"
            elif block[0] == "gate_up":
                stage = "down"
            else:
                rows += block[1]
                sent = max(sent, now) + 0.9
                if len(rows) == RING:
                    stage = "end"
        release()
    return actions, max(now, sent + 4.0)


def wrap(v):
    return lax.rem(v + 2 * RING, RING)


def nt_dot(a, b, precision=None):
    return lax.dot_general(
        a, b, (((1,), (1,)), ((), ())), preferred_element_type=jnp.float32, precision=precision
    )


def layer(
    lam_ref, resid_hbm, q_ref, k_ref, v_ref, hgain_ref, wo_hbm, mgain_ref, gate_ref, up_ref, down_ref, out_ref,
    w0, w1, w2, w3, wo_all, qg, kvg, vext, own_read, own_log, o_part, o_recv, st_part, st_recv, heads_out, heads_all,
    resid, mid, normed, hidden, piece, own_mid, d_own, d_near, d_pair, d_recv,
    ring_ss, ring_rs, last_rs, q_rs, kv_rs, o_rs, st_rs, near_rs, sent, came, local_sem,
):
    sp = lax.axis_index("sp")
    tp = lax.axis_index("tp")
    z = lax.div(sp, RING)
    y = lax.rem(sp, RING)

    def at_zy(zz, yy):
        return {"sp": zz * RING + yy}

    def remote(src, dst, ss, rs, device):
        return pltpu.make_async_remote_copy(
            src_ref=src, dst_ref=dst, send_sem=ss, recv_sem=rs, device_id=device, device_id_type=MESH
        )

    barrier = pltpu.get_barrier_semaphore()
    for d in DIRS:
        pl.semaphore_signal(barrier, inc=1, device_id=at_zy(wrap(z + d), y), device_id_type=MESH)
    for j in range(1, RING):
        pl.semaphore_signal(barrier, inc=1, device_id=at_zy(z, wrap(y + j)), device_id_type=MESH)
        pl.semaphore_signal(barrier, inc=1, device_id={"tp": wrap(tp + j)}, device_id_type=MESH)

    local_resid = pltpu.make_async_copy(resid_hbm, resid, local_sem.at[0])
    local_wo = pltpu.make_async_copy(wo_hbm, wo_all.at[tp], local_sem.at[1])
    local_resid.start()
    local_wo.start()
    qg[y] = q_ref[...]
    kvg[z, 0] = k_ref[...]
    kvg[z, 1] = v_ref[...]
    for c in range(5):
        pair = w0.at[z, y, :, pl.ds(256 * c, 256)] if c < PAIRS else w1.at[z, y, :, pl.ds(256 * (c - PAIRS), 256)]
        pair[:, 0:WIDTH] = gate_ref[:, WIDTH * c : WIDTH * (c + 1)]
        pair[:, WIDTH:] = up_ref[:, WIDTH * c : WIDTH * (c + 1)]
    w1[z, y, :, 256 * (5 - PAIRS) :] = jnp.concatenate([gate_ref[:, 640:], up_ref[:, 640:]], axis=1)
    w2[z, y] = down_ref[:, : PIECES[2][1]]
    w3[z, y, :, : PIECES[3][1] - WIDTH] = down_ref[:, PIECES[2][1] : 640]
    w3[z, y, :, PIECES[3][1] - WIDTH :] = jnp.concatenate([down_ref[:, 640:], jnp.zeros((32, 64), jnp.bfloat16)], axis=1)
    pl.semaphore_wait(barrier, 2 + 2 * (RING - 1))

    flags = own_flags()

    def copy_of(event, arriving=False):
        kind, d, k = event[0], event[-2], event[-1]
        back = k if arriving else k - 1
        if kind == "q":
            slot = qg.at[wrap(y - d * back)]
            index = (d < 0) * 4 + k - 1
            return remote(slot, slot, sent.at[0], q_rs.at[index], at_zy(z, wrap(y + d)))
        if kind == "kv":
            slot = kvg.at[wrap(z - d * back)]
            index = (d < 0) * 4 + k - 1
            return remote(slot, slot, sent.at[1], kv_rs.at[index], at_zy(wrap(z + d), y))
        p = event[1]
        buffer = (w0, w1, w2, w3)[p]
        first_z = PIECES[p][0]
        if kind == "r1":
            dz, dy = (d, 0) if first_z else (0, d)
            slot = buffer.at[wrap(z - dz * back), wrap(y - dy * back)]
            return remote(slot, slot, ring_ss.at[p], ring_rs.at[flags[event]], at_zy(wrap(z + dz), wrap(y + dy)))
        offset = event[2]
        if first_z:
            slot = buffer.at[wrap(z - offset), wrap(y - d * back)]
            device = at_zy(z, wrap(y + d))
        else:
            slot = buffer.at[wrap(z - d * back), wrap(y - offset)]
            device = at_zy(wrap(z + d), y)
        arrived = last_rs.at[p] if last_gate(event) else ring_rs.at[flags[event]]
        return remote(slot, slot, ring_ss.at[4 + p], arrived, device)

    def all_of(ref, ss, rs):
        return remote(ref, ref, ss, rs, {"tp": wrap(tp + 1)})

    def wo_copy(j, slot):
        return remote(wo_hbm, wo_all.at[slot], sent.at[2], came.at[2], {"tp": wrap(tp + 2 * (j + 1))})

    partner = tp + 1 - 2 * lax.rem(tp, 2)

    def core_copy(j, slot):
        return remote(wo_all.at[slot], wo_all.at[slot], sent.at[3], came.at[3], {"tp": partner})

    for j in (0, 2, 1):
        wo_copy(j, tp).start()
    vext[:, WIDTH:] = jnp.ones((RING * ROWS, WIDTH), jnp.bfloat16)

    lane = lax.broadcasted_iota(jnp.int32, (ROWS, WIDTH), 1)
    key_lane = lax.broadcasted_iota(jnp.int32, (1, RING * ROWS), 1)
    key_pos = key_lane + y * ROWS
    for j in range(1, RING):
        key_pos = key_pos + jnp.where(key_lane >= j * ROWS, (RING - 1) * ROWS, 0)
    row_iota = lax.broadcasted_iota(jnp.int32, (ROWS, 1), 0)
    pick = (
        lax.broadcasted_iota(jnp.int32, (8, WIDTH), 1) == 64 * lax.broadcasted_iota(jnp.int32, (8, WIDTH), 0)
    ).astype(jnp.float32)
    spread = (
        lax.div(lax.broadcasted_iota(jnp.int32, (8, 2 * WIDTH), 1), WIDTH)
        == lax.broadcasted_iota(jnp.int32, (8, 2 * WIDTH), 0)
    ).astype(jnp.float32)

    def o_copies(i):
        device = at_zy(z, wrap(y + TURNS[i][0]))
        return (
            remote(o_part.at[i], o_recv.at[i], sent.at[4], o_rs.at[i], device),
            remote(st_part.at[i], st_recv.at[i], sent.at[5], st_rs.at[i], device),
        )

    def attend(i):
        if i == 0:
            vext[:, :WIDTH] = kvg[:, 1].reshape(RING * ROWS, WIDTH)
        d, k = TURNS[i]
        yq = wrap(y + (5 - k if d > 0 else k - 4 if d < 0 else 0))
        q = qg[yq] * jnp.bfloat16(0.125)
        q_pos = z * (RING * ROWS) + yq * ROWS + row_iota
        seen = key_pos <= q_pos
        keys = kvg[:, 0].reshape(RING * ROWS, WIDTH)
        for m in range(2):
            half = (lane < 64) if m == 0 else (lane >= 64)
            qm = jnp.where(half, q.astype(jnp.float32), 0.0).astype(jnp.bfloat16)
            s = jnp.where(seen, nt_dot(qm, keys), FAR)
            top = jnp.max(s, axis=1, keepdims=True)
            p = jnp.exp(s - top).astype(jnp.bfloat16)
            both = jnp.dot(p, vext[...], preferred_element_type=jnp.float32)
            total = both[:, WIDTH:]
            own_read[i, m] = both[:, :WIDTH] / total
            own_log[i, m] = top + jnp.log(total)

    def merged(i, incoming):
        stats = [
            lax.dot_general(st_recv[n], spread, (((0,), (0,)), ((), ())), preferred_element_type=jnp.float32,
                            precision=lax.Precision.HIGHEST) for n in incoming
        ]
        out = []
        for m in range(2):
            logs = [own_log[i, m]] + [st[:, m * WIDTH : (m + 1) * WIDTH] for st in stats]
            reads = [own_read[i, m]] + [o_recv[n, m].astype(jnp.float32) for n in incoming]
            if not incoming:
                out.append((reads[0], logs[0]))
                continue
            top = functools.reduce(jnp.maximum, logs)
            share = [jnp.exp(l - top) for l in logs]
            total = functools.reduce(jnp.add, share)
            read = functools.reduce(jnp.add, [w * o for w, o in zip(share, reads)]) / total
            out.append((read, top + jnp.log(total)))
        return out

    def pass_on(i):
        d, k = TURNS[i]
        out = merged(i, [TURNS.index((d, k - 1))] if k > 1 else [])
        for m in range(2):
            o_part[i, m] = out[m][0].astype(jnp.bfloat16)
        st_part[i] = nt_dot(pick, jnp.where(lane < 64, out[0][1], out[1][1]), lax.Precision.HIGHEST)

    def share_projection():
        local_wo.wait()
        all_of(wo_all.at[pl.ds(0, 3)], sent.at[2], came.at[2]).wait_recv()
        for j in range(4):
            core_copy(j, wrap(tp + 2 * j)).start()

    def h_copy(j, slot):
        lanes = pl.ds(pl.multiple_of(slot * WIDTH, WIDTH), WIDTH)
        return remote(heads_out, heads_all.at[:, lanes], sent.at[6], came.at[6], {"tp": wrap(tp + j + 1)})

    def merge_heads():
        readings = [read for read, _ in merged(7, [TURNS.index((1, 4)), TURNS.index((-1, 3))])]
        diff = readings[0] - lam_ref[0] * readings[1]
        scale = lax.rsqrt(jnp.mean(diff * diff, axis=1, keepdims=True) + 1e-06)
        heads = (diff * scale * hgain_ref[...].astype(jnp.float32)).astype(jnp.bfloat16)
        heads_out[...] = heads
        for j in (2, 3, 4, 1, 5, 0, 6):
            h_copy(j, tp).start()
        heads_all[:, pl.ds(pl.multiple_of(tp * WIDTH, WIDTH), WIDTH)] = heads
        local_resid.wait()

    def project_rows():
        all_of(wo_all.at[pl.ds(0, 4)], sent.at[3], came.at[3]).wait_recv()
        all_of(heads_all.at[:, pl.ds(0, 7 * WIDTH)], sent.at[6], came.at[6]).wait_recv()

        def project(c, squares):
            lanes = pl.ds(pl.multiple_of(c * 256, 256), 256)
            w = wo_all[:, :, lanes].reshape(RING * WIDTH, 256)
            part = jnp.dot(heads_all[...], w, preferred_element_type=jnp.float32)
            m = (resid[:, lanes].astype(jnp.float32) + part).astype(jnp.bfloat16).astype(jnp.float32)
            mid[:, lanes] = m
            return squares + m[:, :WIDTH] * m[:, :WIDTH] + m[:, WIDTH:] * m[:, WIDTH:]

        squares = lax.fori_loop(0, 8, project, jnp.zeros((ROWS, WIDTH), jnp.float32))
        scale = lax.rsqrt(jnp.sum(squares, axis=1, keepdims=True) * (1.0 / MODEL) + 1e-06)

        def norm(c, carry):
            lanes = pl.ds(pl.multiple_of(c * 256, 256), 256)
            normed[:, lanes] = (mid[:, lanes] * scale * mgain_ref[:, lanes].astype(jnp.float32)).astype(jnp.bfloat16)
            return carry

        lax.fori_loop(0, 8, norm, 0)
        for t in range(RING):
            @pl.when(tp == t)
            def _():
                own_mid[...] = mid[t * SHARE : (t + 1) * SHARE, :]

    def silu_times(g, u):
        return (g / (1.0 + jnp.exp(-g)) * u).astype(jnp.bfloat16)

    def gated_rows():
        for p, buffer in ((0, w0), (1, w1)):
            all_of(buffer.at[pl.ds(0, 2)], ring_ss.at[4 + p], last_rs.at[p]).wait_recv()
        for buffer, first, pairs in ((w0, 0, PAIRS), (w1, PAIRS, 5 - PAIRS)):
            def gate_up(c, carry):
                w = buffer[:, :, :, pl.ds(pl.multiple_of(c * 256, 256), 256)].reshape(MODEL, 256)
                r = jnp.dot(normed[...], w, preferred_element_type=jnp.float32)
                lanes = pl.ds(pl.multiple_of((c + first) * WIDTH, WIDTH), WIDTH)
                hidden[:, lanes] = silu_times(r[:, :WIDTH], r[:, WIDTH:])
                return carry

            lax.fori_loop(0, pairs, gate_up, 0)
        r = jnp.dot(normed[...], w1[:, :, :, 256 * (5 - PAIRS) :].reshape(MODEL, WIDTH), preferred_element_type=jnp.float32)
        r = jnp.where(lane < 64, silu_times(r, pltpu.roll(r, 64, 1)).astype(jnp.float32), 0.0)
        hidden[:, 5 * WIDTH :] = r.astype(jnp.bfloat16)

    core = lax.rem(tp, 2)

    def lanes_of(row):
        return pl.ds(pl.multiple_of(wrap(z - row) * 256, 256), 256)

    def near_copy(turn, row):
        src = d_own.at[:, 1 - core, :, lanes_of(row)]
        return remote(src, d_near.at[:, :, lanes_of(row)], sent.at[8], near_rs.at[turn], {"tp": partner})

    def d_copy(j, row):
        peer = wrap(tp + 2 * (j + 1))
        src = d_pair.at[lax.div(peer, 2), :, lanes_of(row)]
        return remote(src, d_recv.at[j, :, lanes_of(row)], sent.at[7], came.at[7], {"tp": peer})

    def add_pair(turn, pair):
        for n, row in enumerate(pair):
            near_copy(2 * turn + n, row).wait_recv()
        for row, q in itertools.product(pair, range(RING // 2)):
            both = d_own[q, core, :, lanes_of(row)].astype(jnp.float32) + d_near[q, :, lanes_of(row)].astype(jnp.float32)
            d_pair[q, :, lanes_of(row)] = both.astype(jnp.bfloat16)
        for row, j in itertools.product(pair, (1, 0, 2)):
            d_copy(j, row).start()

    def down_pair(turn, pair):
        for n, row in enumerate(pair):
            slot = wrap(z - row)
            piece[n] = nt_dot(hidden[:, : PIECES[2][1]], w2[slot].reshape(256, PIECES[2][1])) + nt_dot(
                hidden[:, PIECES[2][1] :], w3[slot].reshape(256, PIECES[3][1])
            )
        for n, row in enumerate(pair):
            for t in range(RING):
                d_own[t // 2, t % 2, :, lanes_of(row)] = piece[n, t * SHARE : (t + 1) * SHARE, :].astype(jnp.bfloat16)
        for n, row in enumerate(pair):
            near_copy(2 * turn + n, row).start()

    turns = []
    for kind, what in plan(LIMITS)[0]:
        if kind == "attend":
            attend(what)
        elif kind == "pass":
            pass_on(what)
        elif kind == "merge":
            share_projection()
            merge_heads()
        elif kind == "project":
            project_rows()
        elif kind == "gate_up":
            gated_rows()
        elif kind == "down":
            down_pair(len(turns), what)
            if turns:
                add_pair(len(turns) - 1, turns[-1])
            turns.append(what)
        elif kind == "wait":
            if what[0] == "o":
                for c in o_copies(TURNS.index(what[1:])):
                    c.wait_recv()
            elif not last_gate(what):
                copy_of(what, True).wait_recv()
        elif what[0] == "o":
            for c in o_copies(TURNS.index(what[1:])):
                c.start()
        else:
            copy_of(what).start()

    add_pair(len(turns) - 1, turns[-1])
    all_of(d_recv, sent.at[7], came.at[7]).wait_recv()
    total = functools.reduce(jnp.add, [d_recv[j].astype(jnp.float32) for j in range(RING // 2 - 1)])
    total = total + d_pair[lax.div(tp, 2)].astype(jnp.float32)
    out_ref[...] = (own_mid[...] + 0.5 * total).astype(jnp.bfloat16)

    for ref, n in (
        (qg.at[pl.ds(0, 7)], 0), (kvg.at[pl.ds(0, 7)], 1), (wo_all.at[pl.ds(0, 3)], 2), (wo_all.at[pl.ds(0, 4)], 3),
        (o_recv, 4), (st_recv, 5), (heads_all.at[:, pl.ds(0, 7 * WIDTH)], 6), (d_recv, 7),
        (d_near, 8),
    ):
        all_of(ref, sent.at[n], came.at[0]).wait_send()
    for p, buffer in enumerate((w0, w1, w2, w3)):
        all_of(buffer.at[0, pl.ds(0, 7)], ring_ss.at[p], last_rs.at[0]).wait_send()
        all_of(buffer.at[pl.ds(0, 7)], ring_ss.at[4 + p], last_rs.at[0]).wait_send()


def local(residual, queries, key_vectors, value_vecs, lambda_head, head_gain, w_out, mlp_gain, w_gate, w_up, w_down):
    vmem = pl.BlockSpec(memory_space=pltpu.VMEM)
    hbm = pl.BlockSpec(memory_space=pl.ANY)
    dma = pltpu.SemaphoreType.DMA
    bf, f32 = jnp.bfloat16, jnp.float32
    return pl.pallas_call(
        layer,
        out_shape=jax.ShapeDtypeStruct((SHARE, MODEL), bf),
        in_specs=[pl.BlockSpec(memory_space=pltpu.SMEM), hbm, vmem, vmem, vmem, vmem, hbm, vmem, vmem, vmem, vmem],
        out_specs=vmem,
        scratch_shapes=[
            *[pltpu.VMEM((RING, RING, 32, lanes), bf) for _, lanes in PIECES],
            pltpu.VMEM((RING, WIDTH, MODEL), bf),
            pltpu.VMEM((RING, ROWS, WIDTH), bf),
            pltpu.VMEM((RING, 2, ROWS, WIDTH), bf),
            pltpu.VMEM((RING * ROWS, 2 * WIDTH), bf),
            pltpu.VMEM((RING, 2, ROWS, WIDTH), f32),
            pltpu.VMEM((RING, 2, ROWS, WIDTH), f32),
            pltpu.VMEM((RING - 1, 2, ROWS, WIDTH), bf),
            pltpu.VMEM((RING - 1, 2, ROWS, WIDTH), bf),
            pltpu.VMEM((RING - 1, 8, ROWS), f32),
            pltpu.VMEM((RING - 1, 8, ROWS), f32),
            pltpu.VMEM((ROWS, WIDTH), bf),
            pltpu.VMEM((ROWS, RING * WIDTH), bf),
            pltpu.VMEM((ROWS, MODEL), bf),
            pltpu.VMEM((ROWS, MODEL), f32),
            pltpu.VMEM((ROWS, MODEL), bf),
            pltpu.VMEM((ROWS, 6 * WIDTH), bf),
            pltpu.VMEM((2, ROWS, 256), f32),
            pltpu.VMEM((SHARE, MODEL), f32),
            pltpu.VMEM((RING // 2, 2, SHARE, MODEL), bf),
            pltpu.VMEM((RING // 2, SHARE, MODEL), bf),
            pltpu.VMEM((RING // 2, SHARE, MODEL), bf),
            pltpu.VMEM((RING // 2 - 1, SHARE, MODEL), bf),
            dma((8,)), dma((len(own_flags()),)), dma((2,)), dma((8,)), dma((8,)), dma((7,)), dma((7,)), dma((8,)), dma((9,)), dma((8,)), dma((2,)),
        ],
        compiler_params=pltpu.CompilerParams(
            collective_id=0, has_side_effects=True, vmem_limit_bytes=56 * 1024 * 1024
        ),
    )(
        lambda_head, residual, queries.reshape(ROWS, WIDTH), key_vectors.reshape(ROWS, WIDTH),
        value_vecs.reshape(ROWS, WIDTH), head_gain.reshape(1, WIDTH), w_out, mlp_gain.reshape(1, MODEL),
        w_gate, w_up, w_down.T,
    )


def solution(mesh):
    in_specs = (
        P("sp", None), P("sp", "tp", None), P("sp", "tp", None), P("sp", "tp", None), P("tp"), P(),
        P("tp", None), P(), P("sp", "tp"), P("sp", "tp"), P("tp", "sp"),
    )
    return jax.shard_map(
        local, mesh=mesh, in_specs=in_specs, out_specs=P(("sp", "tp"), None), check_vma=False
    )
```

```python
import functools
import itertools

import jax
import jax.numpy as jnp
from jax import lax
from jax.experimental import pallas as pl
from jax.experimental.pallas import tpu as pltpu
from jax.sharding import PartitionSpec as P

MESH = pl.DeviceIdType.MESH
RING = 8
ROWS = 160
SHARE = 20
WIDTH = 128
MODEL = 2048
FAR = -1e30
DIRS = (1, -1)
STEPS = {1: 4, -1: 3}
SPREAD = {1: 3, -1: 4}
OFFSETS = (0, 1, -1, 2, -2, 3, -3, -4)
TURNS = ((1, 1), (-1, 1), (1, 2), (-1, 2), (1, 3), (-1, 3), (1, 4), (0, 0))
LIMITS = (1.8, 1.8, 2.5, 2.0)
PAIRS, DOWN = 3, 3
TAIL = 6
DELAY = 2.2
PIECES = ((0, 256 * PAIRS), (1, 1408 - 256 * PAIRS), (0, 128 * DOWN), (1, 768 - 128 * DOWN))


def hops(offset, d):
    return 4 if (d > 0) == (offset % 2 == 0) else 3


def onward(event):
    kind, d, k = event[0], event[-2], event[-1]
    if kind == "o":
        return []
    if kind in ("q", "kv"):
        return [(kind, d, k + 1)] if k < STEPS[d] else []
    if kind == "r1":
        more = [("r1", event[1], d, k + 1)] if k < SPREAD[d] else []
        return more + [("r2", event[1], d * k, e, 1) for e in DIRS]
    return [event[:-1] + (k + 1,)] if k < hops(event[2], d) else []


def last_gate(event):
    return event[0] == "r2" and event[1] < 2 and event[-1] == hops(event[2], event[3])


def own_flags():
    events = [("r1", p, d, k) for p in range(4) for d in DIRS for k in range(1, SPREAD[d] + 1)]
    events += [
        ("r2", p, o, d, k) for p in range(4) for o in OFFSETS for d in DIRS for k in range(1, hops(o, d) + 1)
    ]
    return {e: i for i, e in enumerate(e for e in events if not last_gate(e))}


def over_z(event):
    if event[0] in ("q", "kv", "o"):
        return event[0] == "kv"
    return (PIECES[event[1]][0] == 1) == (event[0] == "r1")


def column_of(event):
    if event[0] not in ("r1", "r2") or event[1] < 2:
        return None
    travel = event[-2] * event[-1]
    along_z = travel if over_z(event) else (event[2] if event[0] == "r2" else 0)
    return along_z % RING


def plan(limits):
    rate, latency = 46600.0, DELAY
    free, arrivals, actions, held = {}, {}, [], []
    now = 0.0
    missing = {r: (14 if r == 0 else 16) for r in range(RING)}
    gated = 2 * (RING * RING - 1)

    def rank(event):
        return 0 if event[0] in ("q", "kv", "o") else 1 + 2 * (event[1] // 2) + (event[0] == "r2")

    def size(event):
        if event[0] in ("q", "kv", "o"):
            return ROWS * WIDTH * (2 if event[0] == "q" else 4)
        return 64 * PIECES[event[1]][1]

    def release():
        for event in sorted(held, key=rank):
            link = (over_z(event), event[-2])
            if stage == "attend" and at is not None and not link[0]:
                calm = limits[1]
            else:
                calm = limits[3] if rank(event) > 2 else limits[0] if at is None else limits[2]
            if rank(event) == 0 or free.get(link, 0.0) - now <= calm:
                held.remove(event)
                free[link] = max(free.get(link, 0.0), now) + size(event) / rate
                arrivals[event] = free[link] + latency
                actions.append(("start", event))

    for d in DIRS:
        held += [("kv", d, 1), ("q", d, 1)]
    for p in range(4):
        held += [("r1", p, d, 1) for d in DIRS] + [("r2", p, 0, d, 1) for d in DIRS]
    attended, passed, stage, at, sent = 0, 0, "attend", None, 0.0
    release()
    came, rows = set(), []
    while arrivals or held or stage != "end":
        if at is None and not any(e[0] in ("q", "kv") for e in list(arrivals) + held):
            at = now
        block = None
        if stage == "attend" and at is not None:
            d, k = TURNS[passed]
            needed = {("o", 1, 4), ("o", -1, 3)} if d == 0 else {("o", d, k - 1)} if k > 1 else set()
            if passed < attended and needed <= came:
                block = ("merge", 0, 1.2) if d == 0 else ("pass", passed, 0.4)
            elif attended < len(TURNS):
                block = ("attend", attended, 1.3)
        elif stage == "project":
            block = ("project", 0, 2.6)
        elif stage == "gate_up" and gated == 0:
            block = ("gate_up", 0, 2.3)
        elif stage == "down":
            done = [r for r in range(RING) if missing[r] == 0 and r not in rows]
            take = 2 if len(rows) < TAIL else 1
            if len(done) >= take:
                block = ("down", tuple(done[:take]), 0.4 * take)
        ready = None if block is None else max(now, at) if stage == "project" else now
        event = min(arrivals, key=lambda e: arrivals[e]) if arrivals else None
        if event is not None and (block is None or arrivals[event] <= ready):
            now = max(now, arrivals.pop(event))
            actions.append(("wait", event))
            came.add(event)
            held += onward(event)
            if column_of(event) is not None:
                missing[column_of(event)] -= 1
            elif event[0] in ("r1", "r2"):
                gated -= 1
        elif block is None:
            now += 0.3
        else:
            now = ready + block[2]
            actions.append(block[:2])
            if block[0] == "attend":
                attended += 1
            elif block[0] == "pass":
                held.append(("o",) + TURNS[passed])
                passed += 1
            elif block[0] == "merge":
                stage, at = "project", now + 5.0
            elif block[0] == "project":
                stage = "gate_up"
            elif block[0] == "gate_up":
                stage = "down"
            else:
                rows += block[1]
                sent = max(sent, now) + 0.45 * len(block[1])
                if len(rows) == RING:
                    stage = "end"
        release()
    return actions, max(now, sent + 4.0)


def wrap(v):
    return lax.rem(v + 2 * RING, RING)


def nt_dot(a, b, precision=None):
    return lax.dot_general(
        a, b, (((1,), (1,)), ((), ())), preferred_element_type=jnp.float32, precision=precision
    )


def layer(
    lam_ref, resid_hbm, q_hbm, k_hbm, v_hbm, hgain_ref, wo_hbm, mgain_ref, gate_hbm, up_hbm, down_hbm, out_ref,
    gate_ref, up_ref, down_ref,
    w0, w1, w2, w3, wo_all, qg, kvg, vext, own_read, own_log, o_part, o_recv, st_part, st_recv, heads_out, heads_all,
    resid, mid, normed, hidden, piece, own_mid, d_own, d_near, d_pair, d_recv,
    ring_ss, ring_rs, last_rs, q_rs, kv_rs, o_rs, st_rs, near_rs, sent, came, local_sem,
):
    sp = lax.axis_index("sp")
    tp = lax.axis_index("tp")
    z = lax.div(sp, RING)
    y = lax.rem(sp, RING)

    def at_zy(zz, yy):
        return {"sp": zz * RING + yy}

    def remote(src, dst, ss, rs, device):
        return pltpu.make_async_remote_copy(
            src_ref=src, dst_ref=dst, send_sem=ss, recv_sem=rs, device_id=device, device_id_type=MESH
        )

    local_copies = [
        pltpu.make_async_copy(src, dst, local_sem.at[n])
        for n, (src, dst) in enumerate((
            (k_hbm, kvg.at[z, 0]), (v_hbm, kvg.at[z, 1]), (q_hbm, qg.at[y]), (gate_hbm, gate_ref), (up_hbm, up_ref),
            (down_hbm, down_ref), (wo_hbm, wo_all.at[tp]), (resid_hbm, resid),
        ))
    ]
    token_copies, weight_copies, (local_wo, local_resid) = local_copies[:3], local_copies[3:6], local_copies[6:]
    for c in local_copies:
        c.start()
    barrier = pltpu.get_barrier_semaphore()
    for d in DIRS:
        pl.semaphore_signal(barrier, inc=1, device_id=at_zy(wrap(z + d), y), device_id_type=MESH)
    for j in range(1, RING):
        pl.semaphore_signal(barrier, inc=1, device_id=at_zy(z, wrap(y + j)), device_id_type=MESH)
        pl.semaphore_signal(barrier, inc=1, device_id={"tp": wrap(tp + j)}, device_id_type=MESH)

    for c in token_copies:
        c.wait()
    pl.semaphore_wait(barrier, 2 + 2 * (RING - 1))

    def pack():
        for c in weight_copies:
            c.wait()
        for c in range(5):
            pair = w0.at[z, y, :, pl.ds(256 * c, 256)] if c < PAIRS else w1.at[z, y, :, pl.ds(256 * (c - PAIRS), 256)]
            pair[:, 0:WIDTH] = gate_ref[:, WIDTH * c : WIDTH * (c + 1)]
            pair[:, WIDTH:] = up_ref[:, WIDTH * c : WIDTH * (c + 1)]
        w1[z, y, :, 256 * (5 - PAIRS) :] = jnp.concatenate([gate_ref[:, 640:], up_ref[:, 640:]], axis=1)
        w2[z, y] = down_ref[:, : PIECES[2][1]]
        w3[z, y, :, : PIECES[3][1] - WIDTH] = down_ref[:, PIECES[2][1] : 640]
        w3[z, y, :, PIECES[3][1] - WIDTH :] = jnp.concatenate(
            [down_ref[:, 640:], jnp.zeros((32, 64), jnp.bfloat16)], axis=1
        )

    flags = own_flags()

    def copy_of(event, arriving=False):
        kind, d, k = event[0], event[-2], event[-1]
        back = k if arriving else k - 1
        if kind == "q":
            slot = qg.at[wrap(y - d * back)]
            index = (d < 0) * 4 + k - 1
            return remote(slot, slot, sent.at[0], q_rs.at[index], at_zy(z, wrap(y + d)))
        if kind == "kv":
            slot = kvg.at[wrap(z - d * back)]
            index = (d < 0) * 4 + k - 1
            return remote(slot, slot, sent.at[1], kv_rs.at[index], at_zy(wrap(z + d), y))
        p = event[1]
        buffer = (w0, w1, w2, w3)[p]
        first_z = PIECES[p][0]
        if kind == "r1":
            dz, dy = (d, 0) if first_z else (0, d)
            slot = buffer.at[wrap(z - dz * back), wrap(y - dy * back)]
            return remote(slot, slot, ring_ss.at[p], ring_rs.at[flags[event]], at_zy(wrap(z + dz), wrap(y + dy)))
        offset = event[2]
        if first_z:
            slot = buffer.at[wrap(z - offset), wrap(y - d * back)]
            device = at_zy(z, wrap(y + d))
        else:
            slot = buffer.at[wrap(z - d * back), wrap(y - offset)]
            device = at_zy(wrap(z + d), y)
        arrived = last_rs.at[p] if last_gate(event) else ring_rs.at[flags[event]]
        return remote(slot, slot, ring_ss.at[4 + p], arrived, device)

    def all_of(ref, ss, rs):
        return remote(ref, ref, ss, rs, {"tp": wrap(tp + 1)})

    def wo_copy(j, slot):
        return remote(wo_hbm, wo_all.at[slot], sent.at[2], came.at[2], {"tp": wrap(tp + 2 * (j + 1))})

    partner = tp + 1 - 2 * lax.rem(tp, 2)

    def core_copy(j, slot):
        return remote(wo_all.at[slot], wo_all.at[slot], sent.at[3], came.at[3], {"tp": partner})

    vext[:, WIDTH:] = jnp.ones((RING * ROWS, WIDTH), jnp.bfloat16)

    lane = lax.broadcasted_iota(jnp.int32, (ROWS, WIDTH), 1)
    key_lane = lax.broadcasted_iota(jnp.int32, (1, RING * ROWS), 1)
    key_pos = key_lane + y * ROWS
    for j in range(1, RING):
        key_pos = key_pos + jnp.where(key_lane >= j * ROWS, (RING - 1) * ROWS, 0)
    row_iota = lax.broadcasted_iota(jnp.int32, (ROWS, 1), 0)
    pick = (
        lax.broadcasted_iota(jnp.int32, (8, WIDTH), 1) == 64 * lax.broadcasted_iota(jnp.int32, (8, WIDTH), 0)
    ).astype(jnp.float32)
    spread = (
        lax.div(lax.broadcasted_iota(jnp.int32, (8, 2 * WIDTH), 1), WIDTH)
        == lax.broadcasted_iota(jnp.int32, (8, 2 * WIDTH), 0)
    ).astype(jnp.float32)

    def o_copies(i):
        device = at_zy(z, wrap(y + TURNS[i][0]))
        return (
            remote(o_part.at[i], o_recv.at[i], sent.at[4], o_rs.at[i], device),
            remote(st_part.at[i], st_recv.at[i], sent.at[5], st_rs.at[i], device),
        )

    def attend(i):
        if i == 0:
            vext[:, :WIDTH] = kvg[:, 1].reshape(RING * ROWS, WIDTH)
        d, k = TURNS[i]
        yq = wrap(y + (5 - k if d > 0 else k - 4 if d < 0 else 0))
        q = qg[yq] * jnp.bfloat16(0.125)
        q_pos = z * (RING * ROWS) + yq * ROWS + row_iota
        seen = key_pos <= q_pos
        keys = kvg[:, 0].reshape(RING * ROWS, WIDTH)
        for m in range(2):
            half = (lane < 64) if m == 0 else (lane >= 64)
            qm = jnp.where(half, q.astype(jnp.float32), 0.0).astype(jnp.bfloat16)
            s = jnp.where(seen, nt_dot(qm, keys), FAR)
            top = jnp.max(s, axis=1, keepdims=True)
            p = jnp.exp(s - top).astype(jnp.bfloat16)
            both = jnp.dot(p, vext[...], preferred_element_type=jnp.float32)
            total = both[:, WIDTH:]
            own_read[i, m] = both[:, :WIDTH] / total
            own_log[i, m] = top + jnp.log(total)

    def merged(i, incoming):
        stats = [
            lax.dot_general(st_recv[n], spread, (((0,), (0,)), ((), ())), preferred_element_type=jnp.float32,
                            precision=lax.Precision.HIGHEST) for n in incoming
        ]
        out = []
        for m in range(2):
            logs = [own_log[i, m]] + [st[:, m * WIDTH : (m + 1) * WIDTH] for st in stats]
            reads = [own_read[i, m]] + [o_recv[n, m].astype(jnp.float32) for n in incoming]
            if not incoming:
                out.append((reads[0], logs[0]))
                continue
            top = functools.reduce(jnp.maximum, logs)
            share = [jnp.exp(l - top) for l in logs]
            total = functools.reduce(jnp.add, share)
            read = functools.reduce(jnp.add, [w * o for w, o in zip(share, reads)]) / total
            out.append((read, top + jnp.log(total)))
        return out

    def pass_on(i):
        d, k = TURNS[i]
        out = merged(i, [TURNS.index((d, k - 1))] if k > 1 else [])
        for m in range(2):
            o_part[i, m] = out[m][0].astype(jnp.bfloat16)
        st_part[i] = nt_dot(pick, jnp.where(lane < 64, out[0][1], out[1][1]), lax.Precision.HIGHEST)

    def share_projection():
        local_wo.wait()
        all_of(wo_all.at[pl.ds(0, 3)], sent.at[2], came.at[2]).wait_recv()
        for j in range(4):
            core_copy(j, wrap(tp + 2 * j)).start()

    def h_copy(j, slot):
        lanes = pl.ds(pl.multiple_of(slot * WIDTH, WIDTH), WIDTH)
        return remote(heads_out, heads_all.at[:, lanes], sent.at[6], came.at[6], {"tp": wrap(tp + j + 1)})

    def merge_heads():
        readings = [read for read, _ in merged(7, [TURNS.index((1, 4)), TURNS.index((-1, 3))])]
        diff = readings[0] - lam_ref[0] * readings[1]
        scale = lax.rsqrt(jnp.mean(diff * diff, axis=1, keepdims=True) + 1e-06)
        heads = (diff * scale * hgain_ref[...].astype(jnp.float32)).astype(jnp.bfloat16)
        heads_out[...] = heads
        for j in (2, 3, 4, 1, 5, 0, 6):
            h_copy(j, tp).start()
        heads_all[:, pl.ds(pl.multiple_of(tp * WIDTH, WIDTH), WIDTH)] = heads
        local_resid.wait()

    def project_rows():
        all_of(wo_all.at[pl.ds(0, 4)], sent.at[3], came.at[3]).wait_recv()
        all_of(heads_all.at[:, pl.ds(0, 7 * WIDTH)], sent.at[6], came.at[6]).wait_recv()

        def project(c, squares):
            lanes = pl.ds(pl.multiple_of(c * 256, 256), 256)
            w = wo_all[:, :, lanes].reshape(RING * WIDTH, 256)
            part = jnp.dot(heads_all[...], w, preferred_element_type=jnp.float32)
            m = (resid[:, lanes].astype(jnp.float32) + part).astype(jnp.bfloat16).astype(jnp.float32)
            mid[:, lanes] = m
            return squares + m[:, :WIDTH] * m[:, :WIDTH] + m[:, WIDTH:] * m[:, WIDTH:]

        squares = lax.fori_loop(0, 8, project, jnp.zeros((ROWS, WIDTH), jnp.float32))
        scale = lax.rsqrt(jnp.sum(squares, axis=1, keepdims=True) * (1.0 / MODEL) + 1e-06)

        gains = mgain_ref[...].astype(jnp.float32)
        for c in range(MODEL // WIDTH):
            lanes = pl.ds(c * WIDTH, WIDTH)
            normed[:, lanes] = (mid[:, lanes] * scale * gains[c : c + 1]).astype(jnp.bfloat16)
        for t in range(RING):
            @pl.when(tp == t)
            def _():
                own_mid[...] = mid[t * SHARE : (t + 1) * SHARE, :]

    def silu_times(g, u):
        return (g / (1.0 + jnp.exp(-g)) * u).astype(jnp.bfloat16)

    def gated_rows():
        for p, buffer in ((0, w0), (1, w1)):
            all_of(buffer.at[pl.ds(0, 2)], ring_ss.at[4 + p], last_rs.at[p]).wait_recv()
        for buffer, first, pairs in ((w0, 0, PAIRS), (w1, PAIRS, 5 - PAIRS)):
            def gate_up(c, carry):
                w = buffer[:, :, :, pl.ds(pl.multiple_of(c * 256, 256), 256)].reshape(MODEL, 256)
                r = jnp.dot(normed[...], w, preferred_element_type=jnp.float32)
                lanes = pl.ds(pl.multiple_of((c + first) * WIDTH, WIDTH), WIDTH)
                hidden[:, lanes] = silu_times(r[:, :WIDTH], r[:, WIDTH:])
                return carry

            lax.fori_loop(0, pairs, gate_up, 0)
        r = jnp.dot(normed[...], w1[:, :, :, 256 * (5 - PAIRS) :].reshape(MODEL, WIDTH), preferred_element_type=jnp.float32)
        r = jnp.where(lane < 64, silu_times(r, pltpu.roll(r, 64, 1)).astype(jnp.float32), 0.0)
        hidden[:, 5 * WIDTH :] = r.astype(jnp.bfloat16)

    core = lax.rem(tp, 2)

    def lanes_of(row):
        return pl.ds(pl.multiple_of(wrap(z - row) * 256, 256), 256)

    def near_copy(turn, row):
        src = d_own.at[:, 1 - core, :, lanes_of(row)]
        return remote(src, d_near.at[:, :, lanes_of(row)], sent.at[8], near_rs.at[turn], {"tp": partner})

    def d_copy(j, row):
        peer = wrap(tp + 2 * (j + 1))
        src = d_pair.at[lax.div(peer, 2), :, lanes_of(row)]
        return remote(src, d_recv.at[j, :, lanes_of(row)], sent.at[7], came.at[7], {"tp": peer})

    def add_pair(turn, pair):
        for n, row in enumerate(pair):
            near_copy(turn + n, row).wait_recv()
        for row, q in itertools.product(pair, range(RING // 2)):
            both = d_own[q, core, :, lanes_of(row)].astype(jnp.float32) + d_near[q, :, lanes_of(row)].astype(jnp.float32)
            d_pair[q, :, lanes_of(row)] = both.astype(jnp.bfloat16)
        for row, j in itertools.product(pair, (1, 0, 2)):
            d_copy(j, row).start()

    def down_pair(turn, pair):
        for n, row in enumerate(pair):
            slot = wrap(z - row)
            piece[n] = nt_dot(hidden[:, : PIECES[2][1]], w2[slot].reshape(256, PIECES[2][1])) + nt_dot(
                hidden[:, PIECES[2][1] :], w3[slot].reshape(256, PIECES[3][1])
            )
        for n, row in enumerate(pair):
            for t in range(RING):
                d_own[t // 2, t % 2, :, lanes_of(row)] = piece[n, t * SHARE : (t + 1) * SHARE, :].astype(jnp.bfloat16)
        for n, row in enumerate(pair):
            near_copy(turn + n, row).start()

    turns, packed = [], False
    for kind, what in plan(LIMITS)[0]:
        if kind == "attend":
            attend(what)
        elif kind == "pass":
            pass_on(what)
        elif kind == "merge":
            share_projection()
            merge_heads()
        elif kind == "project":
            project_rows()
        elif kind == "gate_up":
            gated_rows()
        elif kind == "down":
            down_pair(sum(map(len, turns)), what)
            if turns:
                add_pair(sum(map(len, turns[:-1])), turns[-1])
            turns.append(what)
        elif kind == "wait":
            if what[0] == "o":
                for c in o_copies(TURNS.index(what[1:])):
                    c.wait_recv()
            elif not last_gate(what):
                copy_of(what, True).wait_recv()
        elif what[0] == "o":
            for c in o_copies(TURNS.index(what[1:])):
                c.start()
        else:
            if what[0] in ("r1", "r2") and not packed:
                pack()
                for j in (0, 2, 1):
                    wo_copy(j, tp).start()
                packed = True
            copy_of(what).start()

    add_pair(RING - len(turns[-1]), turns[-1])
    all_of(d_recv, sent.at[7], came.at[7]).wait_recv()
    total = functools.reduce(jnp.add, [d_recv[j].astype(jnp.float32) for j in range(RING // 2 - 1)])
    total = total + d_pair[lax.div(tp, 2)].astype(jnp.float32)
    out_ref[...] = (own_mid[...] + 0.5 * total).astype(jnp.bfloat16)

    for ref, n in (
        (qg.at[pl.ds(0, 7)], 0), (kvg.at[pl.ds(0, 7)], 1), (wo_all.at[pl.ds(0, 3)], 2), (wo_all.at[pl.ds(0, 4)], 3),
        (o_recv, 4), (st_recv, 5), (heads_all.at[:, pl.ds(0, 7 * WIDTH)], 6), (d_recv, 7),
        (d_near, 8),
    ):
        all_of(ref, sent.at[n], came.at[0]).wait_send()
    for p, buffer in enumerate((w0, w1, w2, w3)):
        all_of(buffer.at[0, pl.ds(0, 7)], ring_ss.at[p], last_rs.at[0]).wait_send()
        all_of(buffer.at[pl.ds(0, 7)], ring_ss.at[4 + p], last_rs.at[0]).wait_send()


def local(residual, queries, key_vectors, value_vecs, lambda_head, head_gain, w_out, mlp_gain, w_gate, w_up, w_down):
    vmem = pl.BlockSpec(memory_space=pltpu.VMEM)
    hbm = pl.BlockSpec(memory_space=pl.ANY)
    dma = pltpu.SemaphoreType.DMA
    bf, f32 = jnp.bfloat16, jnp.float32
    return pl.pallas_call(
        layer,
        out_shape=jax.ShapeDtypeStruct((SHARE, MODEL), bf),
        in_specs=[pl.BlockSpec(memory_space=pltpu.SMEM), hbm, hbm, hbm, hbm, vmem, hbm, vmem, hbm, hbm, hbm],
        out_specs=vmem,
        scratch_shapes=[
            pltpu.VMEM((32, 704), bf),
            pltpu.VMEM((32, 704), bf),
            pltpu.VMEM((32, 704), bf),
            *[pltpu.VMEM((RING, RING, 32, lanes), bf) for _, lanes in PIECES],
            pltpu.VMEM((RING, WIDTH, MODEL), bf),
            pltpu.VMEM((RING, ROWS, WIDTH), bf),
            pltpu.VMEM((RING, 2, ROWS, WIDTH), bf),
            pltpu.VMEM((RING * ROWS, 2 * WIDTH), bf),
            pltpu.VMEM((RING, 2, ROWS, WIDTH), f32),
            pltpu.VMEM((RING, 2, ROWS, WIDTH), f32),
            pltpu.VMEM((RING - 1, 2, ROWS, WIDTH), bf),
            pltpu.VMEM((RING - 1, 2, ROWS, WIDTH), bf),
            pltpu.VMEM((RING - 1, 8, ROWS), f32),
            pltpu.VMEM((RING - 1, 8, ROWS), f32),
            pltpu.VMEM((ROWS, WIDTH), bf),
            pltpu.VMEM((ROWS, RING * WIDTH), bf),
            pltpu.VMEM((ROWS, MODEL), bf),
            pltpu.VMEM((ROWS, MODEL), f32),
            pltpu.VMEM((ROWS, MODEL), bf),
            pltpu.VMEM((ROWS, 6 * WIDTH), bf),
            pltpu.VMEM((2, ROWS, 256), f32),
            pltpu.VMEM((SHARE, MODEL), f32),
            pltpu.VMEM((RING // 2, 2, SHARE, MODEL), bf),
            pltpu.VMEM((RING // 2, SHARE, MODEL), bf),
            pltpu.VMEM((RING // 2, SHARE, MODEL), bf),
            pltpu.VMEM((RING // 2 - 1, SHARE, MODEL), bf),
            dma((8,)), dma((len(own_flags()),)), dma((2,)), dma((8,)), dma((8,)), dma((7,)), dma((7,)), dma((8,)), dma((9,)), dma((8,)), dma((8,)),
        ],
        compiler_params=pltpu.CompilerParams(
            collective_id=0, has_side_effects=True, vmem_limit_bytes=56 * 1024 * 1024
        ),
    )(
        lambda_head, residual, queries.reshape(ROWS, WIDTH), key_vectors.reshape(ROWS, WIDTH),
        value_vecs.reshape(ROWS, WIDTH), head_gain.reshape(1, WIDTH), w_out, mlp_gain.reshape(MODEL // WIDTH, WIDTH),
        w_gate, w_up, w_down.T,
    )


def solution(mesh):
    in_specs = (
        P("sp", None), P("sp", "tp", None), P("sp", "tp", None), P("sp", "tp", None), P("tp"), P(),
        P("tp", None), P(), P("sp", "tp"), P("sp", "tp"), P("tp", "sp"),
    )
    return jax.shard_map(
        local, mesh=mesh, in_specs=in_specs, out_specs=P(("sp", "tp"), None), check_vma=False
    )
```

```python
import functools
import itertools

import jax
import jax.numpy as jnp
from jax import lax
from jax.experimental import pallas as pl
from jax.experimental.pallas import tpu as pltpu
from jax.sharding import PartitionSpec as P

MESH = pl.DeviceIdType.MESH
RING = 8
ROWS = 160
SHARE = 20
WIDTH = 128
MODEL = 2048
FAR = -1e30
DIRS = (1, -1)
STEPS = {1: 4, -1: 3}
SPREAD = {1: 3, -1: 4}
OFFSETS = (0, 1, -1, 2, -2, 3, -3, -4)
TURNS = ((1, 1), (-1, 1), (1, 2), (-1, 2), (1, 3), (-1, 3), (1, 4), (0, 0))
LIMITS = (1.8, 1.8, 2.5, 2.0)
PAIRS, DOWN = 3, 3
TAIL = 6
DELAY = 2.2
PIECES = ((0, 256 * PAIRS), (1, 1408 - 256 * PAIRS), (0, 128 * DOWN), (1, 768 - 128 * DOWN))


def hops(offset, d):
    return 4 if (d > 0) == (offset % 2 == 0) else 3


def onward(event):
    kind, d, k = event[0], event[-2], event[-1]
    if kind == "o":
        return []
    if kind in ("q", "kv"):
        return [(kind, d, k + 1)] if k < STEPS[d] else []
    if kind == "r1":
        more = [("r1", event[1], d, k + 1)] if k < SPREAD[d] else []
        return more + [("r2", event[1], d * k, e, 1) for e in DIRS]
    return [event[:-1] + (k + 1,)] if k < hops(event[2], d) else []


def last_gate(event):
    return event[0] == "r2" and event[1] < 2 and event[-1] == hops(event[2], event[3])


def own_flags():
    events = [("r1", p, d, k) for p in range(4) for d in DIRS for k in range(1, SPREAD[d] + 1)]
    events += [
        ("r2", p, o, d, k) for p in range(4) for o in OFFSETS for d in DIRS for k in range(1, hops(o, d) + 1)
    ]
    return {e: i for i, e in enumerate(e for e in events if not last_gate(e))}


def over_z(event):
    if event[0] in ("q", "kv", "o"):
        return event[0] == "kv"
    return (PIECES[event[1]][0] == 1) == (event[0] == "r1")


def column_of(event):
    if event[0] not in ("r1", "r2") or event[1] < 2:
        return None
    travel = event[-2] * event[-1]
    along_z = travel if over_z(event) else (event[2] if event[0] == "r2" else 0)
    return along_z % RING


def plan(limits):
    rate, latency = 46600.0, DELAY
    free, arrivals, actions, held = {}, {}, [], []
    now = 0.0
    missing = {r: (14 if r == 0 else 16) for r in range(RING)}
    gated = 2 * (RING * RING - 1)

    def rank(event):
        return 0 if event[0] in ("q", "kv", "o") else 1 + 2 * (event[1] // 2) + (event[0] == "r2")

    def size(event):
        if event[0] in ("q", "kv", "o"):
            return ROWS * WIDTH * (2 if event[0] == "q" else 4)
        return 64 * PIECES[event[1]][1]

    def release():
        for event in sorted(held, key=rank):
            link = (over_z(event), event[-2])
            if stage == "attend" and at is not None and not link[0]:
                calm = limits[1]
            else:
                calm = limits[3] if rank(event) > 2 else limits[0] if at is None else limits[2]
            if rank(event) == 0 or free.get(link, 0.0) - now <= calm:
                held.remove(event)
                free[link] = max(free.get(link, 0.0), now) + size(event) / rate
                arrivals[event] = free[link] + latency
                actions.append(("start", event))

    for d in DIRS:
        held += [("kv", d, 1), ("q", d, 1)]
    for p in range(4):
        held += [("r1", p, d, 1) for d in DIRS] + [("r2", p, 0, d, 1) for d in DIRS]
    attended, passed, stage, at, sent = 0, 0, "attend", None, 0.0
    release()
    came, rows = set(), []
    while arrivals or held or stage != "end":
        if at is None and not any(e[0] in ("q", "kv") for e in list(arrivals) + held):
            at = now
        block = None
        if stage == "attend" and at is not None:
            d, k = TURNS[passed]
            needed = {("o", 1, 4), ("o", -1, 3)} if d == 0 else {("o", d, k - 1)} if k > 1 else set()
            if passed < attended and needed <= came:
                block = ("merge", 0, 1.2) if d == 0 else ("pass", passed, 0.4)
            elif attended < len(TURNS):
                block = ("attend", attended, 1.3)
        elif stage == "project":
            block = ("project", 0, 2.6)
        elif stage == "gate_up" and gated == 0:
            block = ("gate_up", 0, 2.3)
        elif stage == "down":
            done = [r for r in range(RING) if missing[r] == 0 and r not in rows]
            take = 2 if len(rows) < TAIL else 1
            if len(done) >= take:
                block = ("down", tuple(done[:take]), 0.4 * take)
        ready = None if block is None else max(now, at) if stage == "project" else now
        event = min(arrivals, key=lambda e: arrivals[e]) if arrivals else None
        if event is not None and (block is None or arrivals[event] <= ready):
            now = max(now, arrivals.pop(event))
            actions.append(("wait", event))
            came.add(event)
            held += onward(event)
            if column_of(event) is not None:
                missing[column_of(event)] -= 1
            elif event[0] in ("r1", "r2"):
                gated -= 1
        elif block is None:
            now += 0.3
        else:
            now = ready + block[2]
            actions.append(block[:2])
            if block[0] == "attend":
                attended += 1
            elif block[0] == "pass":
                held.append(("o",) + TURNS[passed])
                passed += 1
            elif block[0] == "merge":
                stage, at = "project", now + 5.0
            elif block[0] == "project":
                stage = "gate_up"
            elif block[0] == "gate_up":
                stage = "down"
            else:
                rows += block[1]
                sent = max(sent, now) + 0.45 * len(block[1])
                if len(rows) == RING:
                    stage = "end"
        release()
    return actions, max(now, sent + 4.0)


def wrap(v):
    return lax.rem(v + 2 * RING, RING)


def nt_dot(a, b, precision=None):
    return lax.dot_general(
        a, b, (((1,), (1,)), ((), ())), preferred_element_type=jnp.float32, precision=precision
    )


def layer(
    lam_ref, resid_hbm, q_hbm, k_hbm, v_hbm, hgain_ref, wo_hbm, mgain_ref, gate_hbm, up_hbm, down_hbm, out_ref,
    gate_ref, up_ref, down_ref,
    w0, w1, w2, w3, wo_all, qg, kvg, vext, own_read, own_log, o_part, o_recv, st_part, st_recv, heads_out, heads_all,
    resid, mid, normed, hidden, piece, own_mid, d_own, d_near, d_pair, d_recv, d_last,
    ring_ss, ring_rs, last_rs, q_rs, kv_rs, o_rs, st_rs, near_rs, sent, came, local_sem,
):
    sp = lax.axis_index("sp")
    tp = lax.axis_index("tp")
    z = lax.div(sp, RING)
    y = lax.rem(sp, RING)

    def at_zy(zz, yy):
        return {"sp": zz * RING + yy}

    def remote(src, dst, ss, rs, device):
        return pltpu.make_async_remote_copy(
            src_ref=src, dst_ref=dst, send_sem=ss, recv_sem=rs, device_id=device, device_id_type=MESH
        )

    local_copies = [
        pltpu.make_async_copy(src, dst, local_sem.at[n])
        for n, (src, dst) in enumerate((
            (k_hbm, kvg.at[z, 0]), (v_hbm, kvg.at[z, 1]), (q_hbm, qg.at[y]), (gate_hbm, gate_ref), (up_hbm, up_ref),
            (down_hbm, down_ref), (wo_hbm, wo_all.at[tp]), (resid_hbm, resid),
        ))
    ]
    token_copies, weight_copies, (local_wo, local_resid) = local_copies[:3], local_copies[3:6], local_copies[6:]
    for c in local_copies:
        c.start()
    barrier = pltpu.get_barrier_semaphore()
    for d in DIRS:
        pl.semaphore_signal(barrier, inc=1, device_id=at_zy(wrap(z + d), y), device_id_type=MESH)
    for j in range(1, RING):
        pl.semaphore_signal(barrier, inc=1, device_id=at_zy(z, wrap(y + j)), device_id_type=MESH)
        pl.semaphore_signal(barrier, inc=1, device_id={"tp": wrap(tp + j)}, device_id_type=MESH)

    for c in token_copies:
        c.wait()
    pl.semaphore_wait(barrier, 2 + 2 * (RING - 1))

    def pack():
        for c in weight_copies:
            c.wait()
        for c in range(5):
            pair = w0.at[z, y, :, pl.ds(256 * c, 256)] if c < PAIRS else w1.at[z, y, :, pl.ds(256 * (c - PAIRS), 256)]
            pair[:, 0:WIDTH] = gate_ref[:, WIDTH * c : WIDTH * (c + 1)]
            pair[:, WIDTH:] = up_ref[:, WIDTH * c : WIDTH * (c + 1)]
        w1[z, y, :, 256 * (5 - PAIRS) :] = jnp.concatenate([gate_ref[:, 640:], up_ref[:, 640:]], axis=1)
        w2[z, y] = down_ref[:, : PIECES[2][1]]
        w3[z, y, :, : PIECES[3][1] - WIDTH] = down_ref[:, PIECES[2][1] : 640]
        w3[z, y, :, PIECES[3][1] - WIDTH :] = jnp.concatenate(
            [down_ref[:, 640:], jnp.zeros((32, 64), jnp.bfloat16)], axis=1
        )

    flags = own_flags()

    def copy_of(event, arriving=False):
        kind, d, k = event[0], event[-2], event[-1]
        back = k if arriving else k - 1
        if kind == "q":
            slot = qg.at[wrap(y - d * back)]
            index = (d < 0) * 4 + k - 1
            return remote(slot, slot, sent.at[0], q_rs.at[index], at_zy(z, wrap(y + d)))
        if kind == "kv":
            slot = kvg.at[wrap(z - d * back)]
            index = (d < 0) * 4 + k - 1
            return remote(slot, slot, sent.at[1], kv_rs.at[index], at_zy(wrap(z + d), y))
        p = event[1]
        buffer = (w0, w1, w2, w3)[p]
        first_z = PIECES[p][0]
        if kind == "r1":
            dz, dy = (d, 0) if first_z else (0, d)
            slot = buffer.at[wrap(z - dz * back), wrap(y - dy * back)]
            return remote(slot, slot, ring_ss.at[p], ring_rs.at[flags[event]], at_zy(wrap(z + dz), wrap(y + dy)))
        offset = event[2]
        if first_z:
            slot = buffer.at[wrap(z - offset), wrap(y - d * back)]
            device = at_zy(z, wrap(y + d))
        else:
            slot = buffer.at[wrap(z - d * back), wrap(y - offset)]
            device = at_zy(wrap(z + d), y)
        arrived = last_rs.at[p] if last_gate(event) else ring_rs.at[flags[event]]
        return remote(slot, slot, ring_ss.at[4 + p], arrived, device)

    def all_of(ref, ss, rs):
        return remote(ref, ref, ss, rs, {"tp": wrap(tp + 1)})

    def wo_copy(j, slot):
        return remote(wo_hbm, wo_all.at[slot], sent.at[2], came.at[2], {"tp": wrap(tp + 2 * (j + 1))})

    partner = tp + 1 - 2 * lax.rem(tp, 2)

    def core_copy(j, slot):
        return remote(wo_all.at[slot], wo_all.at[slot], sent.at[3], came.at[3], {"tp": partner})

    vext[:, WIDTH:] = jnp.ones((RING * ROWS, WIDTH), jnp.bfloat16)

    lane = lax.broadcasted_iota(jnp.int32, (ROWS, WIDTH), 1)
    key_lane = lax.broadcasted_iota(jnp.int32, (1, RING * ROWS), 1)
    key_pos = key_lane + y * ROWS
    for j in range(1, RING):
        key_pos = key_pos + jnp.where(key_lane >= j * ROWS, (RING - 1) * ROWS, 0)
    row_iota = lax.broadcasted_iota(jnp.int32, (ROWS, 1), 0)
    pick = (
        lax.broadcasted_iota(jnp.int32, (8, WIDTH), 1) == 64 * lax.broadcasted_iota(jnp.int32, (8, WIDTH), 0)
    ).astype(jnp.float32)
    spread = (
        lax.div(lax.broadcasted_iota(jnp.int32, (8, 2 * WIDTH), 1), WIDTH)
        == lax.broadcasted_iota(jnp.int32, (8, 2 * WIDTH), 0)
    ).astype(jnp.float32)

    def o_copies(i):
        device = at_zy(z, wrap(y + TURNS[i][0]))
        return (
            remote(o_part.at[i], o_recv.at[i], sent.at[4], o_rs.at[i], device),
            remote(st_part.at[i], st_recv.at[i], sent.at[5], st_rs.at[i], device),
        )

    def attend(i):
        if i == 0:
            vext[:, :WIDTH] = kvg[:, 1].reshape(RING * ROWS, WIDTH)
        d, k = TURNS[i]
        yq = wrap(y + (5 - k if d > 0 else k - 4 if d < 0 else 0))
        q = qg[yq] * jnp.bfloat16(0.125)
        q_pos = z * (RING * ROWS) + yq * ROWS + row_iota
        seen = key_pos <= q_pos
        keys = kvg[:, 0].reshape(RING * ROWS, WIDTH)
        for m in range(2):
            half = (lane < 64) if m == 0 else (lane >= 64)
            qm = jnp.where(half, q.astype(jnp.float32), 0.0).astype(jnp.bfloat16)
            s = jnp.where(seen, nt_dot(qm, keys), FAR)
            top = jnp.max(s, axis=1, keepdims=True)
            p = jnp.exp(s - top).astype(jnp.bfloat16)
            both = jnp.dot(p, vext[...], preferred_element_type=jnp.float32)
            total = both[:, WIDTH:]
            own_read[i, m] = both[:, :WIDTH] / total
            own_log[i, m] = top + jnp.log(total)

    def merged(i, incoming):
        stats = [
            lax.dot_general(st_recv[n], spread, (((0,), (0,)), ((), ())), preferred_element_type=jnp.float32,
                            precision=lax.Precision.HIGHEST) for n in incoming
        ]
        out = []
        for m in range(2):
            logs = [own_log[i, m]] + [st[:, m * WIDTH : (m + 1) * WIDTH] for st in stats]
            reads = [own_read[i, m]] + [o_recv[n, m].astype(jnp.float32) for n in incoming]
            if not incoming:
                out.append((reads[0], logs[0]))
                continue
            top = functools.reduce(jnp.maximum, logs)
            share = [jnp.exp(l - top) for l in logs]
            total = functools.reduce(jnp.add, share)
            read = functools.reduce(jnp.add, [w * o for w, o in zip(share, reads)]) / total
            out.append((read, top + jnp.log(total)))
        return out

    def pass_on(i):
        d, k = TURNS[i]
        out = merged(i, [TURNS.index((d, k - 1))] if k > 1 else [])
        for m in range(2):
            o_part[i, m] = out[m][0].astype(jnp.bfloat16)
        st_part[i] = nt_dot(pick, jnp.where(lane < 64, out[0][1], out[1][1]), lax.Precision.HIGHEST)

    def share_projection():
        local_wo.wait()
        all_of(wo_all.at[pl.ds(0, 3)], sent.at[2], came.at[2]).wait_recv()
        for j in range(4):
            core_copy(j, wrap(tp + 2 * j)).start()

    def h_copy(j, slot):
        lanes = pl.ds(pl.multiple_of(slot * WIDTH, WIDTH), WIDTH)
        return remote(heads_out, heads_all.at[:, lanes], sent.at[6], came.at[6], {"tp": wrap(tp + j + 1)})

    def merge_heads():
        readings = [read for read, _ in merged(7, [TURNS.index((1, 4)), TURNS.index((-1, 3))])]
        diff = readings[0] - lam_ref[0] * readings[1]
        scale = lax.rsqrt(jnp.mean(diff * diff, axis=1, keepdims=True) + 1e-06)
        heads = (diff * scale * hgain_ref[...].astype(jnp.float32)).astype(jnp.bfloat16)
        heads_out[...] = heads
        for j in (2, 3, 4, 1, 5, 0, 6):
            h_copy(j, tp).start()
        heads_all[:, pl.ds(pl.multiple_of(tp * WIDTH, WIDTH), WIDTH)] = heads
        local_resid.wait()

    def project_rows():
        all_of(wo_all.at[pl.ds(0, 4)], sent.at[3], came.at[3]).wait_recv()
        all_of(heads_all.at[:, pl.ds(0, 7 * WIDTH)], sent.at[6], came.at[6]).wait_recv()

        def project(c, squares):
            lanes = pl.ds(pl.multiple_of(c * 256, 256), 256)
            w = wo_all[:, :, lanes].reshape(RING * WIDTH, 256)
            part = jnp.dot(heads_all[...], w, preferred_element_type=jnp.float32)
            m = (resid[:, lanes].astype(jnp.float32) + part).astype(jnp.bfloat16).astype(jnp.float32)
            mid[:, lanes] = m
            return squares + m[:, :WIDTH] * m[:, :WIDTH] + m[:, WIDTH:] * m[:, WIDTH:]

        squares = lax.fori_loop(0, 8, project, jnp.zeros((ROWS, WIDTH), jnp.float32))
        scale = lax.rsqrt(jnp.sum(squares, axis=1, keepdims=True) * (1.0 / MODEL) + 1e-06)

        gains = mgain_ref[...].astype(jnp.float32)
        for c in range(MODEL // WIDTH):
            lanes = pl.ds(c * WIDTH, WIDTH)
            normed[:, lanes] = (mid[:, lanes] * scale * gains[c : c + 1]).astype(jnp.bfloat16)
        for t in range(RING):
            @pl.when(tp == t)
            def _():
                own_mid[...] = mid[t * SHARE : (t + 1) * SHARE, :]

    def silu_times(g, u):
        return (g / (1.0 + jnp.exp(-g)) * u).astype(jnp.bfloat16)

    def gated_rows():
        for p, buffer in ((0, w0), (1, w1)):
            all_of(buffer.at[pl.ds(0, 2)], ring_ss.at[4 + p], last_rs.at[p]).wait_recv()
        for buffer, first, pairs in ((w0, 0, PAIRS), (w1, PAIRS, 5 - PAIRS)):
            def gate_up(c, carry):
                w = buffer[:, :, :, pl.ds(pl.multiple_of(c * 256, 256), 256)].reshape(MODEL, 256)
                r = jnp.dot(normed[...], w, preferred_element_type=jnp.float32)
                lanes = pl.ds(pl.multiple_of((c + first) * WIDTH, WIDTH), WIDTH)
                hidden[:, lanes] = silu_times(r[:, :WIDTH], r[:, WIDTH:])
                return carry

            lax.fori_loop(0, pairs, gate_up, 0)
        r = jnp.dot(normed[...], w1[:, :, :, 256 * (5 - PAIRS) :].reshape(MODEL, WIDTH), preferred_element_type=jnp.float32)
        r = jnp.where(lane < 64, silu_times(r, pltpu.roll(r, 64, 1)).astype(jnp.float32), 0.0)
        hidden[:, 5 * WIDTH :] = r.astype(jnp.bfloat16)

    core = lax.rem(tp, 2)

    def lanes_of(row):
        return pl.ds(pl.multiple_of(wrap(z - row) * 256, 256), 256)

    def near_copy(turn, row):
        src = d_own.at[:, 1 - core, :, lanes_of(row)]
        return remote(src, d_near.at[:, :, lanes_of(row)], sent.at[8], near_rs.at[turn], {"tp": partner})

    def d_copy(j, row):
        peer = wrap(tp + 2 * (j + 1))
        src = d_pair.at[lax.div(peer, 2), :, lanes_of(row)]
        return remote(src, d_recv.at[j, :, lanes_of(row)], sent.at[7], came.at[7], {"tp": peer})

    def last_copy(j, row):
        peer = wrap(tp + j + 1)
        src = d_own.at[lax.div(peer, 2), lax.rem(peer, 2), :, lanes_of(row)]
        return remote(src, d_last.at[j], sent.at[9], came.at[1], {"tp": peer})

    def add_pair(turn, pair):
        for n, row in enumerate(pair):
            near_copy(turn + n, row).wait_recv()
        for row, q in itertools.product(pair, range(RING // 2)):
            both = d_own[q, core, :, lanes_of(row)].astype(jnp.float32) + d_near[q, :, lanes_of(row)].astype(jnp.float32)
            d_pair[q, :, lanes_of(row)] = both.astype(jnp.bfloat16)
        for row, j in itertools.product(pair, (1, 0, 2)):
            d_copy(j, row).start()

    def down_pair(turn, pair):
        for n, row in enumerate(pair):
            slot = wrap(z - row)
            piece[n] = nt_dot(hidden[:, : PIECES[2][1]], w2[slot].reshape(256, PIECES[2][1])) + nt_dot(
                hidden[:, PIECES[2][1] :], w3[slot].reshape(256, PIECES[3][1])
            )
        for n, row in enumerate(pair):
            for t in range(RING):
                d_own[t // 2, t % 2, :, lanes_of(row)] = piece[n, t * SHARE : (t + 1) * SHARE, :].astype(jnp.bfloat16)
        for n, row in enumerate(pair):
            if turn + n == RING - 1:
                for j in (2, 3, 4, 1, 5, 0, 6):
                    last_copy(j, row).start()
            else:
                near_copy(turn + n, row).start()

    turns, packed = [], False
    for kind, what in plan(LIMITS)[0]:
        if kind == "attend":
            attend(what)
        elif kind == "pass":
            pass_on(what)
        elif kind == "merge":
            share_projection()
            merge_heads()
        elif kind == "project":
            project_rows()
        elif kind == "gate_up":
            gated_rows()
        elif kind == "down":
            down_pair(sum(map(len, turns)), what)
            if turns:
                add_pair(sum(map(len, turns[:-1])), turns[-1])
            turns.append(what)
        elif kind == "wait":
            if what[0] == "o":
                for c in o_copies(TURNS.index(what[1:])):
                    c.wait_recv()
            elif not last_gate(what):
                copy_of(what, True).wait_recv()
        elif what[0] == "o":
            for c in o_copies(TURNS.index(what[1:])):
                c.start()
        else:
            if what[0] in ("r1", "r2") and not packed:
                pack()
                for j in (0, 2, 1):
                    wo_copy(j, tp).start()
                packed = True
            copy_of(what).start()

    all_of(d_recv.at[:, :, pl.ds(0, 7 * 256)], sent.at[7], came.at[7]).wait_recv()
    total = functools.reduce(jnp.add, [d_recv[j].astype(jnp.float32) for j in range(RING // 2 - 1)])
    total = total + d_pair[lax.div(tp, 2)].astype(jnp.float32)
    out_ref[...] = (own_mid[...] + 0.5 * total).astype(jnp.bfloat16)
    all_of(d_last, sent.at[9], came.at[1]).wait_recv()
    lanes = lanes_of(turns[-1][-1])
    total = d_own[lax.div(tp, 2), core, :, lanes].astype(jnp.float32)
    total = functools.reduce(jnp.add, [d_last[j].astype(jnp.float32) for j in range(RING - 1)], total)
    out_ref[:, lanes] = (own_mid[:, lanes] + 0.5 * total).astype(jnp.bfloat16)

    for ref, n in (
        (qg.at[pl.ds(0, 7)], 0), (kvg.at[pl.ds(0, 7)], 1), (wo_all.at[pl.ds(0, 3)], 2), (wo_all.at[pl.ds(0, 4)], 3),
        (o_recv, 4), (st_recv, 5), (heads_all.at[:, pl.ds(0, 7 * WIDTH)], 6), (d_recv.at[:, :, pl.ds(0, 7 * 256)], 7),
        (d_near.at[:, :, pl.ds(0, 7 * 256)], 8), (d_last, 9),
    ):
        all_of(ref, sent.at[n], came.at[0]).wait_send()
    for p, buffer in enumerate((w0, w1, w2, w3)):
        all_of(buffer.at[0, pl.ds(0, 7)], ring_ss.at[p], last_rs.at[0]).wait_send()
        all_of(buffer.at[pl.ds(0, 7)], ring_ss.at[4 + p], last_rs.at[0]).wait_send()


def local(residual, queries, key_vectors, value_vecs, lambda_head, head_gain, w_out, mlp_gain, w_gate, w_up, w_down):
    vmem = pl.BlockSpec(memory_space=pltpu.VMEM)
    hbm = pl.BlockSpec(memory_space=pl.ANY)
    dma = pltpu.SemaphoreType.DMA
    bf, f32 = jnp.bfloat16, jnp.float32
    return pl.pallas_call(
        layer,
        out_shape=jax.ShapeDtypeStruct((SHARE, MODEL), bf),
        in_specs=[pl.BlockSpec(memory_space=pltpu.SMEM), hbm, hbm, hbm, hbm, vmem, hbm, vmem, hbm, hbm, hbm],
        out_specs=vmem,
        scratch_shapes=[
            pltpu.VMEM((32, 704), bf),
            pltpu.VMEM((32, 704), bf),
            pltpu.VMEM((32, 704), bf),
            *[pltpu.VMEM((RING, RING, 32, lanes), bf) for _, lanes in PIECES],
            pltpu.VMEM((RING, WIDTH, MODEL), bf),
            pltpu.VMEM((RING, ROWS, WIDTH), bf),
            pltpu.VMEM((RING, 2, ROWS, WIDTH), bf),
            pltpu.VMEM((RING * ROWS, 2 * WIDTH), bf),
            pltpu.VMEM((RING, 2, ROWS, WIDTH), f32),
            pltpu.VMEM((RING, 2, ROWS, WIDTH), f32),
            pltpu.VMEM((RING - 1, 2, ROWS, WIDTH), bf),
            pltpu.VMEM((RING - 1, 2, ROWS, WIDTH), bf),
            pltpu.VMEM((RING - 1, 8, ROWS), f32),
            pltpu.VMEM((RING - 1, 8, ROWS), f32),
            pltpu.VMEM((ROWS, WIDTH), bf),
            pltpu.VMEM((ROWS, RING * WIDTH), bf),
            pltpu.VMEM((ROWS, MODEL), bf),
            pltpu.VMEM((ROWS, MODEL), f32),
            pltpu.VMEM((ROWS, MODEL), bf),
            pltpu.VMEM((ROWS, 6 * WIDTH), bf),
            pltpu.VMEM((2, ROWS, 256), f32),
            pltpu.VMEM((SHARE, MODEL), f32),
            pltpu.VMEM((RING // 2, 2, SHARE, MODEL), bf),
            pltpu.VMEM((RING // 2, SHARE, MODEL), bf),
            pltpu.VMEM((RING // 2, SHARE, MODEL), bf),
            pltpu.VMEM((RING // 2 - 1, SHARE, MODEL), bf),
            pltpu.VMEM((RING - 1, SHARE, 256), bf),
            dma((8,)), dma((len(own_flags()),)), dma((2,)), dma((8,)), dma((8,)), dma((7,)), dma((7,)), dma((8,)), dma((10,)), dma((8,)), dma((8,)),
        ],
        compiler_params=pltpu.CompilerParams(
            collective_id=0, has_side_effects=True, vmem_limit_bytes=56 * 1024 * 1024
        ),
    )(
        lambda_head, residual, queries.reshape(ROWS, WIDTH), key_vectors.reshape(ROWS, WIDTH),
        value_vecs.reshape(ROWS, WIDTH), head_gain.reshape(1, WIDTH), w_out, mlp_gain.reshape(MODEL // WIDTH, WIDTH),
        w_gate, w_up, w_down.T,
    )


def solution(mesh):
    in_specs = (
        P("sp", None), P("sp", "tp", None), P("sp", "tp", None), P("sp", "tp", None), P("tp"), P(),
        P("tp", None), P(), P("sp", "tp"), P("sp", "tp"), P("tp", "sp"),
    )
    return jax.shard_map(
        local, mesh=mesh, in_specs=in_specs, out_specs=P(("sp", "tp"), None), check_vma=False
    )
```
